512 devices in a mesh: sp: 64 (over z, y), tp: 8 (over x, core).
Axes of the slice: x: 4, y: 4, z: 16, core: 2. Of those that a mesh axis runs over, the one named last changes fastest.
Arguments:
- tokens: bfloat16 [16384, 2048], P(('sp', 'tp')), may hold values from -96 to 96
- norm_gain: float32 [2048], replicated, may hold values from 0.1 to 1.9
- w_query: bfloat16 [2048, 1024], P(None, 'tp'), may hold values from -0.3 to 0.3
- w_key: bfloat16 [2048, 1024], P(None, 'tp'), may hold values from -0.3 to 0.3
- w_value: bfloat16 [2048, 1024], P(None, 'tp'), may hold values from -0.125 to 0.125
- w_att_gate: bfloat16 [2048, 1024], P(None, 'tp'), may hold values from -0.125 to 0.125
- w_rec_in: bfloat16 [2048, 1024], P(None, 'tp'), may hold values from -0.125 to 0.125
- w_rec_gate: bfloat16 [2048, 1024], P(None, 'tp'), may hold values from -0.125 to 0.125
- conv_taps: float32 [4, 1024], P(None, 'tp'), may hold values from -3 to 3
- gate_recur: bfloat16 [8, 128, 128], P('tp'), may hold values from -0.5 to 0.5
- gate_input: bfloat16 [8, 128, 128], P('tp'), may hold values from -0.5 to 0.5
- decay_rate: float32 [1024], P('tp'), may hold values from 1e-06 to 0.02
- head_lambda: float32 [8], P('tp'), may hold values from 0.3 to 0.8
- head_gain: float32 [1024], P('tp'), may hold values from 0.1 to 1.9
- out_att: bfloat16 [1024, 2048], P('tp'), may hold values from -0.125 to 0.125
- out_rec: bfloat16 [1024, 2048], P('tp'), may hold values from -0.125 to 0.125
Outputs:
- layer_out: bfloat16 [16384, 2048], P(('sp', 'tp'))
The draws below stay inside these ranges and needn't reach their ends.
All inputs are finite; a program needn't handle non-finite values.
Results may differ from the reference program's by a relative error of at most 0.015.
Values may be sent and summed in bfloat16 or wider, within the bound.
A program may use at most 64 MiB of HBM per device.

```python
import math
import jax
import jax.numpy as jnp
from jax import lax

D = 2048
HEADS = 8
HEAD_DIM = 64
V_DIM = 128
CHANNELS = 1024
GATE_BLOCK = 128
CONV = 4
TOKENS = 16384
BLOCKS = 8


WEIGHT_EDGE = 0.296875


def projection_base(key, salt):
    spread = 1.0 / math.sqrt(D * 4 // 7)
    base = jax.random.truncated_normal(jax.random.fold_in(key, salt), -6.0, 6.0, (D, HEADS * 2 * HEAD_DIM), jnp.float32)
    return jnp.clip(base * spread, -WEIGHT_EDGE, WEIGHT_EDGE)


def draw_w_query(key, part):
    weight = projection_base(key, 7003)
    return weight.astype(jnp.bfloat16)


def draw_w_key(key, part):
    weight = projection_base(key, 7004)
    return weight.astype(jnp.bfloat16)


def draw_tokens(key, part):
    values = jax.random.truncated_normal(jax.random.fold_in(key, 7005), -6.0, 6.0, (TOKENS, D), jnp.float32)
    return values.astype(jnp.bfloat16)


def shard_levels(stream_key, shape, pieces, low, largest):
    def one(dim, parts):
        steps = jax.random.uniform(jax.random.fold_in(jax.random.fold_in(stream_key, 6), dim), (parts,), jnp.float32, low / len(pieces), largest / len(pieces))
        return jnp.repeat(jnp.exp(steps), shape[dim] // parts).reshape((-1,) + (1,) * (len(shape) - dim - 1))

    level = one(*pieces[0])
    for cut in pieces[1:]:
        level = level * one(*cut)
    return level


def gaussian(rng, extent, deviation, reach, shards=(), kind=jnp.bfloat16):
    drawn = jax.random.normal(rng, extent, jnp.float32) * deviation
    if len(shards) > 0:
        drawn = shard_levels(rng, extent, shards, -0.22, 0.18) * drawn
    return jnp.clip(drawn, min=-reach, max=reach).astype(kind)


def setup_inputs(seed: int = 0) -> dict:
    key_list = jax.random.split(jax.random.key(seed), 17)
    tokens = draw_tokens(jax.random.fold_in(key_list[16], 71), 0)
    norm_gain = jnp.clip(1.0 + 0.18 * jax.random.normal(key_list[1], (D,), jnp.float32), 0.1, 1.9)
    w_query = draw_w_query(jax.random.fold_in(key_list[16], 71), 0)
    w_key = draw_w_key(jax.random.fold_in(key_list[16], 71), 0)
    w_value = gaussian(key_list[4], (D, HEADS * V_DIM), D ** -0.5, 0.125, ((1, 8),))
    w_att_gate = gaussian(key_list[5], (D, HEADS * V_DIM), D ** -0.5, 0.125, ((1, 8),))
    w_rec_in = gaussian(key_list[6], (D, CHANNELS), D ** -0.5, 0.125, ((1, 8),))
    w_rec_gate = gaussian(key_list[7], (D, CHANNELS), D ** -0.5, 0.125, ((1, 8),))
    conv_taps = gaussian(key_list[8], (CONV, CHANNELS), CONV ** -0.5, 3.0, ((1, 8),), jnp.float32)
    gate_recur = gaussian(key_list[9], (BLOCKS, GATE_BLOCK, GATE_BLOCK), GATE_BLOCK ** -0.5, 0.5, ((0, 8),))
    gate_input = gaussian(key_list[10], (BLOCKS, GATE_BLOCK, GATE_BLOCK), GATE_BLOCK ** -0.5, 0.5, ((0, 8),))
    decay_rate = jnp.clip(jnp.exp(math.log(0.02) - 9.9034875 * jax.random.uniform(key_list[11], (CHANNELS,), jnp.float32) ** shard_levels(key_list[11], (CHANNELS,), ((0, 8),), -0.2, 0.2)), 9.999999974752427e-07, 0.02)
    head_lambda = jnp.clip(0.3 + 0.5 * jax.random.uniform(key_list[12], (HEADS,), jnp.float32) ** shard_levels(key_list[12], (HEADS,), ((0, 8),), -0.2, 0.2), 0.3, 0.8)
    head_gain = jnp.clip(1.0 + 0.18 * jax.random.normal(key_list[13], (HEADS * V_DIM,), jnp.float32), 0.1, 1.9)
    out_att = gaussian(key_list[14], (HEADS * V_DIM, D), (HEADS * V_DIM + CHANNELS) ** -0.5, 0.125, ((0, 8),))
    out_rec = gaussian(key_list[15], (CHANNELS, D), (HEADS * V_DIM + CHANNELS) ** -0.5, 0.125, ((0, 8),))
    return {"tokens": tokens, "norm_gain": norm_gain, "w_query": w_query, "w_key": w_key, "w_value": w_value, "w_att_gate": w_att_gate, "w_rec_in": w_rec_in, "w_rec_gate": w_rec_gate, "conv_taps": conv_taps, "gate_recur": gate_recur, "gate_input": gate_input, "decay_rate": decay_rate, "head_lambda": head_lambda, "head_gain": head_gain, "out_att": out_att, "out_rec": out_rec}


EPS_INPUT = 1e-06
EPS_HEAD = 1e-05
RATE_SCALE = 8.0
HEAD_FACTOR = 0.8
MASKED = -1e+30

def rms_rows(values, gain, epsilon):
    mean_square = lax.optimization_barrier(jnp.mean(values * values, axis=-1, keepdims=True))
    return values * lax.rsqrt(mean_square + epsilon) * gain

def combine_pair(earlier, later):
    return (earlier[0] * later[0], later[0] * earlier[1] + later[1])

def reference(tokens, norm_gain, w_query, w_key, w_value, w_att_gate, w_rec_in, w_rec_gate, conv_taps, gate_recur, gate_input, decay_rate, head_lambda, head_gain, out_att, out_rec):
    normed = rms_rows(tokens.astype(jnp.float32), norm_gain, EPS_INPUT).astype(jnp.bfloat16)

    def project(weight):
        return jnp.dot(normed, weight, preferred_element_type=jnp.float32).astype(jnp.bfloat16)
    queries = project(w_query).reshape(TOKENS, HEADS, 2, HEAD_DIM)
    keys = project(w_key).reshape(TOKENS, HEADS, 2, HEAD_DIM)
    values = project(w_value).reshape(TOKENS, HEADS, V_DIM)
    att_gate = project(w_att_gate)
    rec_in = project(w_rec_in)
    rec_gate = project(w_rec_gate)
    block_rows = math.gcd(TOKENS, 512)
    scale = HEAD_DIM ** (-0.5)
    key_pos = jnp.arange(TOKENS, dtype=jnp.int32)

    def one_head(operands):
        head_query, head_key, head_value, weight_lambda = operands

        def one_block(index):
            anchor = (index * block_rows).astype(jnp.int32)
            query_block = lax.dynamic_slice_in_dim(head_query, anchor, block_rows, 0)
            query_pos = anchor + jnp.arange(block_rows, dtype=jnp.int32)
            allowed = key_pos[None, :] <= query_pos[:, None]

            def weighted_of(which):
                scores = jnp.dot(query_block[:, which], head_key[:, which].T, preferred_element_type=jnp.float32) * scale
                scores = jnp.where(allowed, scores, MASKED)
                top = lax.optimization_barrier(jnp.max(scores, axis=-1, keepdims=True))
                raised = jnp.where(allowed, jnp.exp(scores - top), 0.0)
                total = lax.optimization_barrier(jnp.sum(raised, axis=-1, keepdims=True))
                weighted = jnp.dot(raised.astype(jnp.bfloat16), head_value, preferred_element_type=jnp.float32)
                return weighted / total
            return weighted_of(0) - weight_lambda * weighted_of(1)
        blocks = lax.map(one_block, jnp.arange(TOKENS // block_rows, dtype=jnp.int32))
        return blocks.reshape(TOKENS, V_DIM)
    per_head = lax.map(one_head, (jnp.moveaxis(queries, 1, 0), jnp.moveaxis(keys, 1, 0), jnp.moveaxis(values, 1, 0), head_lambda))
    head_out = rms_rows(per_head, head_gain.reshape(HEADS, 1, V_DIM), EPS_HEAD) * HEAD_FACTOR
    head_out = jnp.moveaxis(head_out, 0, 1).reshape(TOKENS, HEADS * V_DIM)
    att_mixed = (head_out * jax.nn.silu(att_gate.astype(jnp.float32))).astype(jnp.bfloat16)
    padded = jnp.concatenate([jnp.zeros((CONV - 1, CHANNELS), jnp.bfloat16), rec_in], axis=0).astype(jnp.float32)
    conv_sum = jnp.zeros((TOKENS, CHANNELS), jnp.float32)
    for offset in range(CONV):
        conv_sum = conv_sum + padded[offset:offset + TOKENS] * conv_taps[offset]
    conv_out = conv_sum.astype(jnp.bfloat16)
    grouped = conv_out.reshape(TOKENS, BLOCKS, GATE_BLOCK).astype(jnp.float32)
    recur_gate = jax.nn.sigmoid(jnp.einsum('tnc,ncd->tnd', grouped, gate_recur.astype(jnp.float32)).reshape(TOKENS, CHANNELS))
    inflow = jax.nn.sigmoid(jnp.einsum('tnc,ncd->tnd', grouped, gate_input.astype(jnp.float32)).reshape(TOKENS, CHANNELS))
    log_decay = -RATE_SCALE * recur_gate * decay_rate
    decays = jnp.exp(log_decay)
    at_anchor = (jnp.arange(TOKENS, dtype=jnp.int32) == 0)[:, None]
    norm_in = jnp.where(at_anchor, 1.0, jnp.sqrt(-jnp.expm1(2.0 * log_decay)))
    driven = norm_in * inflow * conv_out.astype(jnp.float32)
    _, states = lax.associative_scan(combine_pair, (decays, driven), axis=0)
    rec_mixed = (states * jax.nn.silu(rec_gate.astype(jnp.float32))).astype(jnp.bfloat16)
    output = jnp.dot(att_mixed, out_att, preferred_element_type=jnp.float32) + jnp.dot(rec_mixed, out_rec, preferred_element_type=jnp.float32)
    return output.astype(jnp.bfloat16)
```

```python
import functools
import math

import jax
import jax.numpy as jnp
from jax import lax
from jax.experimental import pallas as pl
from jax.experimental.pallas import tpu as pltpu
from jax.sharding import PartitionSpec as P

MESH = pl.DeviceIdType.MESH
F32 = jnp.float32
BF16 = jnp.bfloat16

EPS_INPUT = 1e-06
EPS_HEAD = 1e-05
RATE_SCALE = 8.0
HEAD_FACTOR = 0.8
MASKED = -1e30
LOG2E = math.log2(math.e)
WIDTH = 128


def minus_expm1(x):
    series = 1.0 + x * (
        1 / 2 + x * (1 / 6 + x * (1 / 24 + x * (1 / 120 + x * (1 / 720 + x * (1 / 5040)))))
    )
    return jnp.where(x > -0.5, -x * series, 1.0 - jnp.exp(x))


def kernel(
    Z, Y, X,
    tokens, norm_gain, w_query, w_key, w_value, w_att_gate, w_rec_in, w_rec_gate, conv_taps,
    gate_recur, gate_input, decay_rate, head_lambda, head_gain, out_att, out_rec,
    out,
    wcat, wout, xbuf, kbuf, vbuf, qbuf, qext, acc, m_ref, l_ref, gate_s, rec_s, recg_s, halo, ext,
    prods, parts, yagg, zagg, stat, cbuf, pbuf, own_c, mixed, ptx, prx, own_o, rtx, rrx,
    w_sem, ag_s, ag_r, kv_s, kv_r, q_s, q_r, halo_s, halo_r, ya_s, ya_r, za_s, za_r,
    st_s, st_r, cb_s, cb_r, pr_s, pr_r, rs_s, rs_r,
):
    rows = tokens.shape[0]
    R = xbuf.shape[0]
    H, G = Z // 2, Z - 1 - Z // 2
    sp, tp = lax.axis_index("sp"), lax.axis_index("tp")
    z, y = sp // Y, sp % Y
    x, c = tp // 2, tp % 2
    way = 1 - 2 * c
    x_fwd, x_bwd, x_far = (x + way + X) % X, (x - way + X) % X, (x + 2) % X
    partner = (sp, 2 * x + 1 - c)
    fwd, bwd = (sp, 2 * x_fwd + c), (sp, 2 * x_bwd + c)
    z_up, z_down = (((z + 1) % Z) * Y + y, tp), (((z + Z - 1) % Z) * Y + y, tp)
    sp_next, sp_prev = ((sp + 1) % (Z * Y), tp), ((sp + Z * Y - 1) % (Z * Y), tp)

    def plane(d):
        return (z * Y + (y + d) % Y, tp)

    def remote(src, dst, send, recv, device):
        return pltpu.make_async_remote_copy(
            src_ref=src, dst_ref=dst, send_sem=send, recv_sem=recv,
            device_id=device, device_id_type=MESH,
        )

    loads = [
        pltpu.make_async_copy(w, wcat.at[:, i * WIDTH : (i + 1) * WIDTH], w_sem.at[i])
        for i, w in enumerate((w_key, w_value, w_query, w_att_gate, w_rec_in, w_rec_gate))
    ]
    loads += [
        pltpu.make_async_copy(w, wout.at[i * WIDTH : (i + 1) * WIDTH, :], w_sem.at[6 + i])
        for i, w in enumerate((out_att, out_rec))
    ]
    for load in loads:
        load.start()

    barrier = pltpu.get_barrier_semaphore()
    peers = [partner, fwd, bwd, z_up, z_down, sp_next, sp_prev] + [plane(d) for d in range(1, Y)]
    for peer in peers:
        pl.semaphore_signal(barrier, inc=1, device_id=peer, device_id_type=MESH)

    tok = tokens[...].astype(F32)
    scale = lax.rsqrt(jnp.mean(tok * tok, axis=-1, keepdims=True) + EPS_INPUT)
    xbuf[pl.ds(pl.multiple_of(tp * rows, rows), rows), :] = (tok * scale * norm_gain[...]).astype(BF16)

    pl.semaphore_wait(barrier, len(peers))

    def ag(slot, device, k):
        piece = xbuf.at[pl.ds(pl.multiple_of(slot * rows, rows), rows), :]
        return remote(piece, piece, ag_s.at[k], ag_r.at[slot], device)

    sent = []

    def send(copy):
        copy.start()
        sent.append(copy)

    send(ag(tp, fwd, 0))
    send(ag(tp, bwd, 1))
    send(ag(tp, partner, 2))
    ag(2 * x_bwd + c, fwd, 3).wait_recv()
    send(ag(2 * x_bwd + c, fwd, 3))
    send(ag(2 * x_bwd + c, partner, 4))
    ag(2 * x_fwd + c, partner, 5).wait_recv()
    send(ag(2 * x_fwd + c, partner, 5))
    ag(2 * x_far + c, partner, 6).wait_recv()
    send(ag(2 * x_far + c, partner, 6))
    for i in range(X):
        ag(2 * i + 1 - c, partner, 6).wait_recv()

    for load in loads[:2]:
        load.wait()
    normed = xbuf[...]
    kv = jnp.dot(normed, wcat[:, : 2 * WIDTH], preferred_element_type=F32)
    kbuf[z] = kv[:, :WIDTH].astype(BF16)
    vbuf[z] = kv[:, WIDTH:].T.astype(BF16)

    bufs = (kbuf, vbuf)

    def ring(way_, kind, slot, step):
        piece = bufs[kind].at[slot]
        return remote(
            piece, piece, kv_s.at[2 * way_ + kind, step], kv_r.at[kind, slot],
            (z_up, z_down)[way_],
        )

    for kind in range(2):
        ring(0, kind, z, 0).start()
        if G > 0:
            ring(1, kind, z, 0).start()

    for load in loads[2:4]:
        load.wait()
    qg = jnp.dot(normed, wcat[:, 2 * WIDTH : 4 * WIDTH], preferred_element_type=F32)
    qbuf[y] = qg[:, :WIDTH].T.astype(BF16)
    for d in range(1, Y):
        send(remote(qbuf.at[y], qbuf.at[y], q_s.at[d], q_r.at[y], plane(d)))
    gate_s[...] = qg[:, WIDTH:].astype(BF16)

    for load in loads[4:]:
        load.wait()
    rr = jnp.dot(normed, wcat[:, 4 * WIDTH :], preferred_element_type=F32)
    rec_s[...] = rr[:, :WIDTH].astype(BF16)
    send(remote(rec_s.at[R - 16 :, :], halo, halo_s, halo_r, sp_next))
    recg_s[...] = rr[:, WIDTH:].astype(BF16)

    row = lax.broadcasted_iota(jnp.int32, (R, WIDTH), 0)

    remote(halo, halo, halo_s, halo_r, sp_next).wait_recv()
    ext[0:16, :] = jnp.where(sp > 0, halo[...].astype(F32), 0.0)
    ext[16:, :] = rec_s[...].astype(F32)
    conv = jnp.zeros((R, WIDTH), F32)
    for j in range(4):
        conv = conv + ext[13 + j : 13 + j + R, :] * conv_taps[j : j + 1, :]
    conv_out = conv.astype(BF16)
    recur = jax.nn.sigmoid(jnp.dot(conv_out, gate_recur[0], preferred_element_type=F32))
    inflow = jax.nn.sigmoid(jnp.dot(conv_out, gate_input[0], preferred_element_type=F32))
    log_decay = -RATE_SCALE * recur * decay_rate[...]
    first = jnp.logical_and(row == 0, sp == 0)
    factor = jnp.where(first, 1.0, jnp.sqrt(minus_expm1(2.0 * log_decay)))
    a = jnp.exp(log_decay)
    b = factor * inflow * conv_out.astype(F32)
    k = 1
    while k < R:
        inside = row >= k
        b = b + a * jnp.where(inside, pltpu.roll(b, k, 0), 0.0)
        a = a * jnp.where(inside, pltpu.roll(a, k, 0), 1.0)
        k *= 2
    prods[...] = a
    parts[...] = b
    sub = lax.broadcasted_iota(jnp.int32, (8, WIDTH), 0)
    yagg[y] = jnp.where(sub == 0, a[R - 1 : R, :], b[R - 1 : R, :])
    for d in range(1, Y):
        send(remote(yagg.at[y], yagg.at[y], ya_s.at[d], ya_r.at[y], plane(d)))

    def plane_total():
        for d in range(1, Y):
            src = (y + d) % Y
            remote(yagg.at[src], yagg.at[src], ya_s.at[0], ya_r.at[src], plane(d)).wait_recv()
        ta, tb = yagg[0, 0:1, :], yagg[0, 1:2, :]
        for i in range(1, Y):
            ia, ib = yagg[i, 0:1, :], yagg[i, 1:2, :]
            ta, tb = ia * ta, ia * tb + ib
        zagg[z] = jnp.where(sub == 0, ta, tb)
        state(0, z, 0).start()
        if G > 0:
            state(1, z, 0).start()

    def state(way_, slot, step):
        piece = zagg.at[slot]
        return remote(piece, piece, za_s.at[way_, step], za_r.at[slot], (z_up, z_down)[way_])

    def state_step(j):
        up, down = (z - j + Z) % Z, (z + j) % Z
        state(0, up, 0).wait_recv()

        @pl.when(j < H)
        def _():
            state(0, up, j).start()

        @pl.when(j <= G)
        def _():
            state(1, down, 0).wait_recv()

            @pl.when(j < G)
            def _():
                state(1, down, j).start()

    def tile(slot, opening):
        key = kbuf[slot]
        keys = jnp.concatenate([key, key], axis=1)
        value = vbuf[slot]
        for i in range(2 * Y):
            s = jnp.dot(keys, qext[i], preferred_element_type=F32)
            if opening:
                pos = lax.broadcasted_iota(jnp.int32, (R, R), 1) - lax.broadcasted_iota(
                    jnp.int32, (R, R), 0
                )
                allowed = pos + (i // 2 - y) * R >= 0
                s = jnp.where(allowed, s, MASKED)
                top = jnp.max(s, axis=0, keepdims=True)
                p = jnp.where(allowed, jnp.exp2(s - top), 0.0)
                l_ref[i : i + 1, :] = jnp.sum(p, axis=0, keepdims=True)
                acc[i] = jnp.dot(value, p.astype(BF16), preferred_element_type=F32)
            else:
                old = m_ref[i : i + 1, :]
                top = jnp.maximum(old, jnp.max(s, axis=0, keepdims=True))
                p = jnp.exp2(s - top)
                fade = jnp.exp2(old - top)
                l_ref[i : i + 1, :] = l_ref[i : i + 1, :] * fade + jnp.sum(p, axis=0, keepdims=True)
                acc[i] = acc[i] * fade + jnp.dot(value, p.astype(BF16), preferred_element_type=F32)
            m_ref[i : i + 1, :] = top

    def opening():
        for d in range(1, Y):
            src = (y + d) % Y
            remote(qbuf.at[src], qbuf.at[src], q_s.at[0], q_r.at[src], plane(d)).wait_recv()
        half = WIDTH // 2
        none = jnp.zeros((half, R), BF16)
        for i in range(Y):
            q = qbuf[i].astype(F32) * (LOG2E * half ** -0.5)
            high = q.astype(BF16)
            low = (q - high.astype(F32)).astype(BF16)
            qext[2 * i] = jnp.concatenate([high[:half], none, low[:half], none], axis=0)
            qext[2 * i + 1] = jnp.concatenate([none, high[half:], none, low[half:]], axis=0)
        tile(z, True)

    def step(s, carry):
        up, down = (z - s + Z) % Z, (z + s) % Z
        for kind in range(2):
            ring(0, kind, up, 0).wait_recv()

            @pl.when(s < H)
            def _():
                ring(0, kind, up, s).start()

            @pl.when(s <= G)
            def _():
                ring(1, kind, down, 0).wait_recv()

                @pl.when(s < G)
                def _():
                    ring(1, kind, down, s).start()

        @pl.when(s == 1)
        def _():
            opening()

        @pl.when(s == 2)
        def _():
            plane_total()

        @pl.when(s > 2)
        def _():
            state_step(s - 2)

        @pl.when(z >= s)
        def _():
            tile(up, False)

        @pl.when(jnp.logical_and(s <= G, z + s >= Z))
        def _():
            tile(down, False)

        return carry

    lax.fori_loop(1, H + 1, step, 0)

    stat[y, 0 : 2 * Y, :] = m_ref[0 : 2 * Y, :]
    stat[y, 2 * Y : 4 * Y, :] = l_ref[0 : 2 * Y, :]
    for d in range(1, Y):
        send(remote(stat.at[y], stat.at[y], st_s.at[d], st_r.at[y], plane(d)))
    for d in range(1, Y):
        src = (y + d) % Y
        remote(stat.at[src], stat.at[src], st_s.at[0], st_r.at[src], plane(d)).wait_recv()
    lam = head_lambda[...]

    def comb_copy(i):
        return remote(cbuf.at[i], pbuf.at[y], cb_s.at[i], cb_r.at[y], (z * Y + i, tp))

    for i in range(Y):
        weight = []
        for n in (2 * i, 2 * i + 1):
            tops = [stat[j, n : n + 1, :] for j in range(Y)]
            top = functools.reduce(jnp.maximum, tops)
            total = sum(stat[j, 2 * Y + n : 2 * Y + n + 1, :] * jnp.exp2(tops[j] - top) for j in range(Y))
            weight.append(jnp.exp2(m_ref[n : n + 1, :] - top) / total)
        comb = acc[2 * i] * weight[0] - acc[2 * i + 1] * (weight[1] * lam)

        @pl.when(y == i)
        def _():
            own_c[...] = comb

        @pl.when(y != i)
        def _():
            cbuf[i] = comb.astype(BF16)
            comb_copy(i).start()

    def late(j, carry):
        state_step(j)
        return carry

    lax.fori_loop(max(H - 1, 1), H + 1, late, 0)
    h = jnp.zeros((1, WIDTH), F32)
    for i in range(Z - 1):
        h = jnp.where(i < z, zagg[i, 0:1, :] * h + zagg[i, 1:2, :], h)
    for i in range(Y - 1):
        h = jnp.where(i < y, yagg[i, 0:1, :] * h + yagg[i, 1:2, :], h)
    states = parts[...] + prods[...] * h
    recg = recg_s[...].astype(F32)
    mixed[:, WIDTH:] = (states * (recg * jax.nn.sigmoid(recg))).astype(BF16)

    total = own_c[...]
    for d in range(1, Y):
        src = (y + d) % Y
        remote(pbuf.at[src], pbuf.at[src], cb_s.at[0], cb_r.at[src], plane(d)).wait_recv()
        total = total + pbuf[src].astype(F32)
    total = total * lax.rsqrt(jnp.mean(total * total, axis=0, keepdims=True) + EPS_HEAD)
    gate = gate_s[...].astype(F32)
    att = total.T * head_gain[...] * HEAD_FACTOR * (gate * jax.nn.sigmoid(gate))
    mixed[:, :WIDTH] = att.astype(BF16)

    def group(core):
        return jnp.concatenate(
            [
                mixed[pl.ds(pl.multiple_of((2 * i + core) * rows, rows), rows), :]
                for i in range(X)
            ],
            axis=0,
        )

    wo = wout[...]
    ptx[...] = jnp.dot(group(1 - c), wo, preferred_element_type=F32).astype(BF16).reshape(ptx.shape)
    send(remote(ptx, prx, pr_s, pr_r, partner))
    own_o[...] = jnp.dot(group(c), wo, preferred_element_type=F32).reshape(own_o.shape)
    remote(ptx, prx, pr_s, pr_r, partner).wait_recv()

    def both(i):
        return own_o[i] + prx[i].astype(F32)

    def hop(k, device):
        return remote(rtx.at[k], rrx.at[k], rs_s.at[k], rs_r.at[k], device)

    rtx[0] = both(x_far).astype(BF16)
    send(hop(0, fwd))
    rtx[1] = both(x_bwd).astype(BF16)
    send(hop(1, bwd))
    hop(0, fwd).wait_recv()
    rtx[2] = (both(x_fwd) + rrx[0].astype(F32)).astype(BF16)
    send(hop(2, fwd))
    hop(1, bwd).wait_recv()
    mine = both(x) + rrx[1].astype(F32)
    hop(2, fwd).wait_recv()
    out[...] = (mine + rrx[2].astype(F32)).astype(BF16)

    for copy in sent:
        copy.wait_send()
    for i in range(Y):

        @pl.when(y != i)
        def _():
            comb_copy(i).wait_send()

    def drain(s, carry):
        for kind in range(2):
            ring(0, kind, z, s).wait_send()

            @pl.when(s < G)
            def _():
                ring(1, kind, z, s).wait_send()

        state(0, z, s).wait_send()

        @pl.when(s < G)
        def _():
            state(1, z, s).wait_send()

        return carry

    lax.fori_loop(0, H, drain, 0)


def build(mesh, Y):
    SP, TP = mesh.shape["sp"], mesh.shape["tp"]
    Z, X = SP // Y, TP // 2

    def body(
        tokens, norm_gain, w_query, w_key, w_value, w_att_gate, w_rec_in, w_rec_gate, conv_taps,
        gate_recur, gate_input, decay_rate, head_lambda, head_gain, out_att, out_rec,
    ):
        rows, D = tokens.shape
        R = rows * TP
        H, G = Z // 2, max(Z - 1 - Z // 2, 1)
        vmem, far = pl.BlockSpec(memory_space=pltpu.VMEM), pl.BlockSpec(memory_space=pl.ANY)
        V, dma = pltpu.VMEM, pltpu.SemaphoreType.DMA
        scratch = [
            V((D, 6 * WIDTH), BF16), V((2 * WIDTH, D), BF16), V((R, D), BF16),
            V((Z, R, WIDTH), BF16), V((Z, WIDTH, R), BF16), V((Y, WIDTH, R), BF16),
            V((2 * Y, 2 * WIDTH, R), BF16), V((2 * Y, WIDTH, R), F32),
            V((2 * Y, R), F32), V((2 * Y, R), F32),
            V((R, WIDTH), BF16), V((R, WIDTH), BF16), V((R, WIDTH), BF16),
            V((16, WIDTH), BF16), V((R + 16, WIDTH), F32),
            V((R, WIDTH), F32), V((R, WIDTH), F32), V((Y, 8, WIDTH), F32), V((Z, 8, WIDTH), F32),
            V((Y, 4 * Y, R), F32), V((Y, WIDTH, R), BF16), V((Y, WIDTH, R), BF16),
            V((WIDTH, R), F32), V((R, 2 * WIDTH), BF16),
            V((X, rows, D), BF16), V((X, rows, D), BF16), V((X, rows, D), F32),
            V((3, rows, D), BF16), V((3, rows, D), BF16),
            dma((8,)), dma((7,)), dma((TP,)), dma((4, H)), dma((2, Z)), dma((Y,)), dma((Y,)),
            dma(()), dma(()), dma((Y,)), dma((Y,)), dma((2, H)), dma((Z,)),
            dma((Y,)), dma((Y,)), dma((Y,)), dma((Y,)), dma(()), dma(()), dma((3,)), dma((3,)),
        ]
        return pl.pallas_call(
            functools.partial(kernel, Z, Y, X),
            out_shape=jax.ShapeDtypeStruct((rows, D), BF16),
            in_specs=[vmem, vmem] + [far] * 6 + [vmem] * 6 + [far] * 2,
            out_specs=vmem,
            scratch_shapes=scratch,
            compiler_params=pltpu.CompilerParams(
                collective_id=0, has_side_effects=True, vmem_limit_bytes=56 * 1024 * 1024
            ),
        )(
            tokens, norm_gain.reshape(1, -1), w_query, w_key, w_value, w_att_gate, w_rec_in,
            w_rec_gate, conv_taps, gate_recur, gate_input, decay_rate.reshape(1, -1),
            head_lambda.reshape(1, 1), head_gain.reshape(1, -1), out_att, out_rec,
        )

    both = P(("sp", "tp"), None)
    cols, lead = P(None, "tp"), P("tp")
    placed = (
        both, P(), cols, cols, cols, cols, cols, cols, cols,
        P("tp", None, None), P("tp", None, None), lead, lead, lead, P("tp", None), P("tp", None),
    )
    return jax.shard_map(body, mesh=mesh, in_specs=placed, out_specs=both, check_vma=False)


def solution(mesh):
    return build(mesh, 4)
```

```python
import functools
import math

import jax
import jax.numpy as jnp
from jax import lax
from jax.experimental import pallas as pl
from jax.experimental.pallas import tpu as pltpu
from jax.sharding import PartitionSpec as P

MESH = pl.DeviceIdType.MESH
F32 = jnp.float32
BF16 = jnp.bfloat16

EPS_INPUT = 1e-06
EPS_HEAD = 1e-05
RATE_SCALE = 8.0
HEAD_FACTOR = 0.8
MASKED = -1e30
LOG2E = math.log2(math.e)
PIECES = 4
HALVES = 2
WIDTH = 128


def minus_expm1(x):
    series = 1.0 + x * (
        1 / 2 + x * (1 / 6 + x * (1 / 24 + x * (1 / 120 + x * (1 / 720 + x * (1 / 5040)))))
    )
    return jnp.where(x > -0.5, -x * series, 1.0 - jnp.exp(x))


def kernel(
    Z, Y, X,
    tokens, norm_gain, w_query, w_key, w_value, w_att_gate, w_rec_in, w_rec_gate, conv_taps,
    gate_recur, gate_input, decay_rate, head_lambda, head_gain, out_att, out_rec,
    out,
    wcat, wout, xbuf, kbuf, vbuf, qbuf, qext, acc, m_ref, l_ref, gate_s, rec_s, recg_s, halo, ext,
    prods, parts, yagg, zagg, stat, cbuf, pbuf, own_c, mixed, ptx, prx, own_o, rtx, rrx,
    w_sem, ag_s, ag_r, kv_s, kv_r, q_s, q_r, halo_s, halo_r, ya_s, ya_r, za_s, za_r,
    st_s, st_r, cb_s, cb_r, pr_s, pr_r, rs_s, rs_r,
):
    rows = tokens.shape[0]
    R = xbuf.shape[0]
    H, G = Z // 2, Z - 1 - Z // 2
    wide = tokens.shape[1] // PIECES
    sp, tp = lax.axis_index("sp"), lax.axis_index("tp")
    z, y = sp // Y, sp % Y
    x, c = tp // 2, tp % 2
    way = 1 - 2 * c
    x_fwd, x_bwd, x_far = (x + way + X) % X, (x - way + X) % X, (x + 2) % X
    partner = (sp, 2 * x + 1 - c)
    fwd, bwd = (sp, 2 * x_fwd + c), (sp, 2 * x_bwd + c)
    z_up, z_down = (((z + 1) % Z) * Y + y, tp), (((z + Z - 1) % Z) * Y + y, tp)
    sp_next, sp_prev = ((sp + 1) % (Z * Y), tp), ((sp + Z * Y - 1) % (Z * Y), tp)

    def plane(d):
        return (z * Y + (y + d) % Y, tp)

    def remote(src, dst, send, recv, device):
        return pltpu.make_async_remote_copy(
            src_ref=src, dst_ref=dst, send_sem=send, recv_sem=recv,
            device_id=device, device_id_type=MESH,
        )

    loads = [
        pltpu.make_async_copy(w, wcat.at[:, i * WIDTH : (i + 1) * WIDTH], w_sem.at[i])
        for i, w in enumerate((w_key, w_value, w_query, w_att_gate, w_rec_in, w_rec_gate))
    ]
    loads += [
        pltpu.make_async_copy(w, wout.at[i * WIDTH : (i + 1) * WIDTH, :], w_sem.at[6 + i])
        for i, w in enumerate((out_att, out_rec))
    ]
    for load in loads:
        load.start()

    barrier = pltpu.get_barrier_semaphore()
    peers = [partner, fwd, bwd, z_up, z_down, sp_next, sp_prev] + [plane(d) for d in range(1, Y)]
    for peer in peers:
        pl.semaphore_signal(barrier, inc=1, device_id=peer, device_id_type=MESH)

    tok = tokens[...].astype(F32)
    scale = lax.rsqrt(jnp.mean(tok * tok, axis=-1, keepdims=True) + EPS_INPUT)
    xbuf[pl.ds(pl.multiple_of(tp * rows, rows), rows), :] = (tok * scale * norm_gain[...]).astype(BF16)

    pl.semaphore_wait(barrier, len(peers))

    def ag(slot, device, k, part):
        piece = xbuf.at[
            pl.ds(pl.multiple_of(slot * rows, rows), rows), part * wide : (part + 1) * wide
        ]
        return remote(piece, piece, ag_s.at[k, part], ag_r.at[slot, part], device)

    sent = []

    def send(copy):
        copy.start()
        sent.append(copy)
        return copy

    parts_x = range(PIECES)
    heads = [send(ag(tp, fwd, 0, q)) for q in parts_x]
    for q in parts_x:
        send(ag(tp, partner, 1, q))
    for copy in heads:
        copy.wait_send()
        sent.remove(copy)
    for q in parts_x:
        send(ag(tp, bwd, 2, q))
    for q in parts_x:
        ag(2 * x_bwd + c, fwd, 3, q).wait_recv()
        send(ag(2 * x_bwd + c, fwd, 3, q))
    for q in parts_x:
        send(ag(2 * x_bwd + c, partner, 4, q))
    for slot, k in ((2 * x_fwd + c, 5), (2 * x_far + c, 6)):
        for q in parts_x:
            ag(slot, partner, k, q).wait_recv()
            send(ag(slot, partner, k, q))
    for i in range(X):
        for q in parts_x:
            ag(2 * i + 1 - c, partner, 6, q).wait_recv()

    for load in loads[:2]:
        load.wait()
    normed = xbuf[...]
    kv = jnp.dot(normed, wcat[:, : 2 * WIDTH], preferred_element_type=F32)
    kbuf[z] = kv[:, :WIDTH].astype(BF16)
    vbuf[z] = kv[:, WIDTH:].T.astype(BF16)

    bufs = (kbuf, vbuf)

    def ring(way_, kind, slot, step):
        half = bufs[kind // HALVES].shape[1] // HALVES
        at = kind % HALVES * half
        piece = bufs[kind // HALVES].at[slot, at : at + half, :]
        return remote(
            piece, piece, kv_s.at[way_, kind, step], kv_r.at[kind, slot], (z_up, z_down)[way_]
        )

    kinds = list(range(2 * HALVES))
    for kind in kinds:
        ring(0, kind, z, 0).start()
        if G > 0:
            ring(1, kind, z, 0).start()

    for load in loads[2:4]:
        load.wait()
    qg = jnp.dot(normed, wcat[:, 2 * WIDTH : 4 * WIDTH], preferred_element_type=F32)
    qbuf[y] = qg[:, :WIDTH].T.astype(BF16)
    for d in range(1, Y):
        send(remote(qbuf.at[y], qbuf.at[y], q_s.at[d], q_r.at[y], plane(d)))
    gate_s[...] = qg[:, WIDTH:].astype(BF16)

    for load in loads[4:]:
        load.wait()
    rr = jnp.dot(normed, wcat[:, 4 * WIDTH :], preferred_element_type=F32)
    rec_s[...] = rr[:, :WIDTH].astype(BF16)
    send(remote(rec_s.at[R - 16 :, :], halo, halo_s, halo_r, sp_next))
    recg_s[...] = rr[:, WIDTH:].astype(BF16)


    sub = lax.broadcasted_iota(jnp.int32, (8, WIDTH), 0)

    def block_scan():
        row = lax.broadcasted_iota(jnp.int32, (R, WIDTH), 0)
        remote(halo, halo, halo_s, halo_r, sp_next).wait_recv()
        ext[0:16, :] = jnp.where(sp > 0, halo[...].astype(F32), 0.0)
        ext[16:, :] = rec_s[...].astype(F32)
        conv = jnp.zeros((R, WIDTH), F32)
        for j in range(4):
            conv = conv + ext[13 + j : 13 + j + R, :] * conv_taps[j : j + 1, :]
        conv_out = conv.astype(BF16)
        recur = jax.nn.sigmoid(jnp.dot(conv_out, gate_recur[0], preferred_element_type=F32))
        inflow = jax.nn.sigmoid(jnp.dot(conv_out, gate_input[0], preferred_element_type=F32))
        log_decay = -RATE_SCALE * recur * decay_rate[...]
        first = jnp.logical_and(row == 0, sp == 0)
        factor = jnp.where(first, 1.0, jnp.sqrt(minus_expm1(2.0 * log_decay)))
        a = jnp.exp(log_decay)
        b = factor * inflow * conv_out.astype(F32)
        k = 1
        while k < R:
            inside = row >= k
            b = b + a * jnp.where(inside, pltpu.roll(b, k, 0), 0.0)
            a = a * jnp.where(inside, pltpu.roll(a, k, 0), 1.0)
            k *= 2
        prods[...] = a
        parts[...] = b
        yagg[y] = jnp.where(sub == 0, a[R - 1 : R, :], b[R - 1 : R, :])
        for d in range(1, Y):
            agg_copy(d).start()
        return

    def agg_copy(d):
        return remote(yagg.at[y], yagg.at[y], ya_s.at[d], ya_r.at[y], plane(d))

    def plane_total():
        for d in range(1, Y):
            src = (y + d) % Y
            remote(yagg.at[src], yagg.at[src], ya_s.at[0], ya_r.at[src], plane(d)).wait_recv()
        ta, tb = yagg[0, 0:1, :], yagg[0, 1:2, :]
        for i in range(1, Y):
            ia, ib = yagg[i, 0:1, :], yagg[i, 1:2, :]
            ta, tb = ia * ta, ia * tb + ib
        zagg[z] = jnp.where(sub == 0, ta, tb)
        state(0, z, 0).start()
        if G > 0:
            state(1, z, 0).start()

    def state(way_, slot, step):
        piece = zagg.at[slot]
        return remote(piece, piece, za_s.at[way_, step], za_r.at[slot], (z_up, z_down)[way_])

    def state_step(j):
        up, down = (z - j + Z) % Z, (z + j) % Z
        state(0, up, 0).wait_recv()

        @pl.when(j < H)
        def _():
            state(0, up, j).start()

        @pl.when(j <= G)
        def _():
            state(1, down, 0).wait_recv()

            @pl.when(j < G)
            def _():
                state(1, down, j).start()

    def tile(slot, opening):
        key = kbuf[slot]
        keys = jnp.concatenate([key, key], axis=1)
        value = vbuf[slot]
        n = 2 * Y
        score = lambda i: jnp.dot(keys, qext[i], preferred_element_type=F32)
        scores = [score(i) for i in range(n)]

        for i in range(n):
            s = scores[i]
            if opening:
                pos = lax.broadcasted_iota(jnp.int32, (R, R), 1) - lax.broadcasted_iota(
                    jnp.int32, (R, R), 0
                )
                allowed = pos + (i // 2 - y) * R >= 0
                s = jnp.where(allowed, s, MASKED)
                top = jnp.max(s, axis=0, keepdims=True)
                p = jnp.where(allowed, jnp.exp2(s - top), 0.0)
                l_ref[i : i + 1, :] = jnp.sum(p, axis=0, keepdims=True)
                acc[i] = jnp.dot(value, p.astype(BF16), preferred_element_type=F32)
            else:
                old = m_ref[i : i + 1, :]
                top = jnp.maximum(old, jnp.max(s, axis=0, keepdims=True))
                p = jnp.exp2(s - top)
                fade = jnp.exp2(old - top)
                l_ref[i : i + 1, :] = l_ref[i : i + 1, :] * fade + jnp.sum(p, axis=0, keepdims=True)
                acc[i] = acc[i] * fade + jnp.dot(value, p.astype(BF16), preferred_element_type=F32)
            m_ref[i : i + 1, :] = top

    def opening():
        for d in range(1, Y):
            src = (y + d) % Y
            remote(qbuf.at[src], qbuf.at[src], q_s.at[0], q_r.at[src], plane(d)).wait_recv()
        half = WIDTH // 2
        none = jnp.zeros((half, R), BF16)
        for i in range(Y):
            q = qbuf[i].astype(F32) * (LOG2E * half ** -0.5)
            high = q.astype(BF16)
            low = (q - high.astype(F32)).astype(BF16)
            qext[2 * i] = jnp.concatenate([high[:half], none, low[:half], none], axis=0)
            qext[2 * i + 1] = jnp.concatenate([none, high[half:], none, low[half:]], axis=0)
        tile(z, True)

    def pass_on(s, some):
        up, down = (z - s + Z) % Z, (z + s) % Z
        for kind in some:
            ring(0, kind, up, 0).wait_recv()

            @pl.when(s < H)
            def _():
                ring(0, kind, up, s).start()

            @pl.when(s <= G)
            def _():
                ring(1, kind, down, 0).wait_recv()

                @pl.when(s < G)
                def _():
                    ring(1, kind, down, s).start()

    def step(s, carry):
        pass_on(s, kinds[:HALVES])

        @pl.when(s == 1)
        def _():
            block_scan()

        @pl.when(jnp.logical_and(s > 1, z >= s - 1))
        def _():
            tile((z - s + 1 + Z) % Z, False)

        pass_on(s, kinds[HALVES:])

        @pl.when(s == 1)
        def _():
            opening()

        @pl.when(jnp.logical_and(s > 1, z + s - 1 >= Z))
        def _():
            tile((z + s - 1) % Z, False)

        @pl.when(s == 2)
        def _():
            plane_total()

        @pl.when(s > 2)
        def _():
            state_step(s - 2)

        return carry

    lax.fori_loop(1, H + 1, step, 0)

    @pl.when(z >= H)
    def _():
        tile(z - H, False)

    stat[y, 0 : 2 * Y, :] = m_ref[0 : 2 * Y, :]
    stat[y, 2 * Y : 4 * Y, :] = l_ref[0 : 2 * Y, :]
    for d in range(1, Y):
        send(remote(stat.at[y], stat.at[y], st_s.at[d], st_r.at[y], plane(d)))
    if H > 1:
        state_step(H - 1)
    for d in range(1, Y):
        src = (y + d) % Y
        remote(stat.at[src], stat.at[src], st_s.at[0], st_r.at[src], plane(d)).wait_recv()
    lam = head_lambda[...]

    def comb_copy(i):
        return remote(cbuf.at[i], pbuf.at[y], cb_s.at[i], cb_r.at[y], (z * Y + i, tp))

    for i in range(Y):
        weight = []
        for n in (2 * i, 2 * i + 1):
            tops = [stat[j, n : n + 1, :] for j in range(Y)]
            top = functools.reduce(jnp.maximum, tops)
            total = sum(stat[j, 2 * Y + n : 2 * Y + n + 1, :] * jnp.exp2(tops[j] - top) for j in range(Y))
            weight.append(jnp.exp2(m_ref[n : n + 1, :] - top) / total)
        comb = acc[2 * i] * weight[0] - acc[2 * i + 1] * (weight[1] * lam)

        @pl.when(y == i)
        def _():
            own_c[...] = comb

        @pl.when(y != i)
        def _():
            cbuf[i] = comb.astype(BF16)
            comb_copy(i).start()

    state_step(H)
    h = jnp.zeros((1, WIDTH), F32)
    for i in range(Z - 1):
        h = jnp.where(i < z, zagg[i, 0:1, :] * h + zagg[i, 1:2, :], h)
    for i in range(Y - 1):
        h = jnp.where(i < y, yagg[i, 0:1, :] * h + yagg[i, 1:2, :], h)
    states = parts[...] + prods[...] * h
    recg = recg_s[...].astype(F32)
    mixed[:, WIDTH:] = (states * (recg * jax.nn.sigmoid(recg))).astype(BF16)

    total = own_c[...]
    for d in range(1, Y):
        src = (y + d) % Y
        remote(pbuf.at[src], pbuf.at[src], cb_s.at[0], cb_r.at[src], plane(d)).wait_recv()
        total = total + pbuf[src].astype(F32)
    total = total * lax.rsqrt(jnp.mean(total * total, axis=0, keepdims=True) + EPS_HEAD)
    gate = gate_s[...].astype(F32)
    att = total.T * head_gain[...] * HEAD_FACTOR * (gate * jax.nn.sigmoid(gate))
    mixed[:, :WIDTH] = att.astype(BF16)

    def group(core):
        return jnp.concatenate(
            [
                mixed[pl.ds(pl.multiple_of((2 * i + core) * rows, rows), rows), :]
                for i in range(X)
            ],
            axis=0,
        )

    def cols(q):
        return slice(q * wide, (q + 1) * wide)

    def swap(q):
        return remote(ptx.at[:, :, cols(q)], prx.at[:, :, cols(q)], pr_s.at[q], pr_r.at[q], partner)

    theirs, ours = group(1 - c), group(c)
    for q in parts_x:
        part = jnp.dot(theirs, wout[:, cols(q)], preferred_element_type=F32)
        ptx[:, :, cols(q)] = part.astype(BF16).reshape(X, rows, wide)
        send(swap(q))
    for q in parts_x:
        part = jnp.dot(ours, wout[:, cols(q)], preferred_element_type=F32)
        own_o[:, :, cols(q)] = part.reshape(X, rows, wide)

    def both(i, q):
        return own_o[i, :, cols(q)] + prx[i, :, cols(q)].astype(F32)

    def hop(k, q, device):
        return remote(
            rtx.at[k, :, cols(q)], rrx.at[k, :, cols(q)], rs_s.at[k, q], rs_r.at[k, q], device
        )

    for q in parts_x:
        swap(q).wait_recv()
        rtx[0, :, cols(q)] = both(x_far, q).astype(BF16)
        send(hop(0, q, fwd))
    for q in parts_x:
        rtx[1, :, cols(q)] = both(x_bwd, q).astype(BF16)
        send(hop(1, q, bwd))
    for q in parts_x:
        hop(0, q, fwd).wait_recv()
        rtx[2, :, cols(q)] = (both(x_fwd, q) + rrx[0, :, cols(q)].astype(F32)).astype(BF16)
        send(hop(2, q, fwd))
    for q in parts_x:
        hop(1, q, bwd).wait_recv()
        mine = both(x, q) + rrx[1, :, cols(q)].astype(F32)
        hop(2, q, fwd).wait_recv()
        out[:, cols(q)] = (mine + rrx[2, :, cols(q)].astype(F32)).astype(BF16)

    for copy in sent:
        copy.wait_send()
    for d in range(1, Y):
        agg_copy(d).wait_send()
    for i in range(Y):

        @pl.when(y != i)
        def _():
            comb_copy(i).wait_send()

    def drain(s, carry):
        for kind in kinds:
            ring(0, kind, z, s).wait_send()

            @pl.when(s < G)
            def _():
                ring(1, kind, z, s).wait_send()

        state(0, z, s).wait_send()

        @pl.when(s < G)
        def _():
            state(1, z, s).wait_send()

        return carry

    lax.fori_loop(0, H, drain, 0)


def build(mesh, Y):
    SP, TP = mesh.shape["sp"], mesh.shape["tp"]
    Z, X = SP // Y, TP // 2

    def body(
        tokens, norm_gain, w_query, w_key, w_value, w_att_gate, w_rec_in, w_rec_gate, conv_taps,
        gate_recur, gate_input, decay_rate, head_lambda, head_gain, out_att, out_rec,
    ):
        rows, D = tokens.shape
        R = rows * TP
        H, G = Z // 2, max(Z - 1 - Z // 2, 1)
        vmem, far = pl.BlockSpec(memory_space=pltpu.VMEM), pl.BlockSpec(memory_space=pl.ANY)
        V, dma = pltpu.VMEM, pltpu.SemaphoreType.DMA
        scratch = [
            V((D, 6 * WIDTH), BF16), V((2 * WIDTH, D), BF16), V((R, D), BF16),
            V((Z, R, WIDTH), BF16), V((Z, WIDTH, R), BF16), V((Y, WIDTH, R), BF16),
            V((2 * Y, 2 * WIDTH, R), BF16), V((2 * Y, WIDTH, R), F32),
            V((2 * Y, R), F32), V((2 * Y, R), F32),
            V((R, WIDTH), BF16), V((R, WIDTH), BF16), V((R, WIDTH), BF16),
            V((16, WIDTH), BF16), V((R + 16, WIDTH), F32),
            V((R, WIDTH), F32), V((R, WIDTH), F32), V((Y, 8, WIDTH), F32), V((Z, 8, WIDTH), F32),
            V((Y, 4 * Y, R), F32), V((Y, WIDTH, R), BF16), V((Y, WIDTH, R), BF16),
            V((WIDTH, R), F32), V((R, 2 * WIDTH), BF16),
            V((X, rows, D), BF16), V((X, rows, D), BF16), V((X, rows, D), F32),
            V((3, rows, D), BF16), V((3, rows, D), BF16),
            dma((8,)), dma((7, PIECES)), dma((TP, PIECES)), dma((2, 2 * HALVES, H)), dma((2 * HALVES, Z)), dma((Y,)), dma((Y,)),
            dma(()), dma(()), dma((Y,)), dma((Y,)), dma((2, H)), dma((Z,)),
            dma((Y,)), dma((Y,)), dma((Y,)), dma((Y,)), dma((PIECES,)), dma((PIECES,)), dma((3, PIECES)), dma((3, PIECES)),
        ]
        return pl.pallas_call(
            functools.partial(kernel, Z, Y, X),
            out_shape=jax.ShapeDtypeStruct((rows, D), BF16),
            in_specs=[vmem, vmem] + [far] * 6 + [vmem] * 6 + [far] * 2,
            out_specs=vmem,
            scratch_shapes=scratch,
            compiler_params=pltpu.CompilerParams(
                collective_id=0, has_side_effects=True, vmem_limit_bytes=56 * 1024 * 1024
            ),
        )(
            tokens, norm_gain.reshape(1, -1), w_query, w_key, w_value, w_att_gate, w_rec_in,
            w_rec_gate, conv_taps, gate_recur, gate_input, decay_rate.reshape(1, -1),
            head_lambda.reshape(1, 1), head_gain.reshape(1, -1), out_att, out_rec,
        )

    both = P(("sp", "tp"), None)
    cols, lead = P(None, "tp"), P("tp")
    placed = (
        both, P(), cols, cols, cols, cols, cols, cols, cols,
        P("tp", None, None), P("tp", None, None), lead, lead, lead, P("tp", None), P("tp", None),
    )
    return jax.shard_map(body, mesh=mesh, in_specs=placed, out_specs=both, check_vma=False)


def solution(mesh):
    return build(mesh, 4)
```

```python
import functools
import math

import jax
import jax.numpy as jnp
from jax import lax
from jax.experimental import pallas as pl
from jax.experimental.pallas import tpu as pltpu
from jax.sharding import PartitionSpec as P

MESH = pl.DeviceIdType.MESH
F32 = jnp.float32
BF16 = jnp.bfloat16

EPS_INPUT = 1e-06
EPS_HEAD = 1e-05
RATE_SCALE = 8.0
HEAD_FACTOR = 0.8
MASKED = -1e30
LOG2E = math.log2(math.e)
PIECES = 4
HALVES = 2
WIDTH = 128


def minus_expm1(x):
    series = 1.0 + x * (
        1 / 2 + x * (1 / 6 + x * (1 / 24 + x * (1 / 120 + x * (1 / 720 + x * (1 / 5040)))))
    )
    return jnp.where(x > -0.5, -x * series, 1.0 - jnp.exp(x))


def kernel(
    Z, Y, X,
    tokens, norm_gain, w_query, w_key, w_value, w_att_gate, w_rec_in, w_rec_gate, conv_taps,
    gate_recur, gate_input, decay_rate, head_lambda, head_gain, out_att, out_rec,
    out,
    wcat, wfull, xbuf, kbuf, vbuf, qbuf, qext, acc, m_ref, l_ref, last_p, last_f, gate_s, rec_s, recg_s, halo, ext,
    prods, parts, yagg, zagg, stat, cbuf, pbuf, own_c, att_m, rec_m, att_g, rec_g, out_a,
    w_sem, ag_s, ag_r, ag_p, kv_s, kv_r, q_s, q_r, halo_s, halo_r, ya_s, ya_r, za_s, za_r,
    st_s, st_r, cb_s, cb_r, wg_s, wg_r, wg_p, am_s, am_r, rm_s, rm_r,
):
    rows = tokens.shape[0]
    R = xbuf.shape[0]
    H, G = Z // 2, Z - 1 - Z // 2
    wide = tokens.shape[1] // PIECES
    sp, tp = lax.axis_index("sp"), lax.axis_index("tp")
    z, y = sp // Y, sp % Y
    x, c = tp // 2, tp % 2
    way = 1 - 2 * c
    x_fwd, x_bwd, x_far = (x + way + X) % X, (x - way + X) % X, (x + 2) % X
    partner = (sp, 2 * x + 1 - c)
    fwd, bwd = (sp, 2 * x_fwd + c), (sp, 2 * x_bwd + c)
    z_up, z_down = (((z + 1) % Z) * Y + y, tp), (((z + Z - 1) % Z) * Y + y, tp)
    sp_next, sp_prev = ((sp + 1) % (Z * Y), tp), ((sp + Z * Y - 1) % (Z * Y), tp)

    def plane(d):
        return (z * Y + (y + d) % Y, tp)

    def row_peer(d):
        return (sp, (tp + d) % (2 * X))

    def remote(src, dst, send, recv, device):
        return pltpu.make_async_remote_copy(
            src_ref=src, dst_ref=dst, send_sem=send, recv_sem=recv,
            device_id=device, device_id_type=MESH,
        )

    def all_sent(piece, sem):
        remote(piece, piece, sem, sem, partner).wait_send()

    def all_here(piece, sem):
        remote(piece, piece, sem, sem, partner).wait_recv()

    loads = [
        pltpu.make_async_copy(w, wcat.at[:, i * WIDTH : (i + 1) * WIDTH], w_sem.at[i])
        for i, w in enumerate((w_key, w_value, w_query, w_att_gate, w_rec_in, w_rec_gate))
    ]
    loads += [
        pltpu.make_async_copy(
            w, wfull.at[i, pl.ds(pl.multiple_of(tp * WIDTH, WIDTH), WIDTH), :], w_sem.at[6 + i]
        )
        for i, w in enumerate((out_rec, out_att))
    ]
    for load in loads:
        load.start()

    barrier = pltpu.get_barrier_semaphore()
    peers = [z_up, z_down, sp_next, sp_prev] + [plane(d) for d in range(1, Y)]
    peers += [row_peer(d) for d in range(1, 2 * X)]
    for peer in peers:
        pl.semaphore_signal(barrier, inc=1, device_id=peer, device_id_type=MESH)

    tok = tokens[...].astype(F32)
    scale = lax.rsqrt(jnp.mean(tok * tok, axis=-1, keepdims=True) + EPS_INPUT)
    xbuf[pl.ds(pl.multiple_of(tp * rows, rows), rows), :] = (tok * scale * norm_gain[...]).astype(BF16)

    pl.semaphore_wait(barrier, len(peers))

    def block(slot):
        return xbuf.at[pl.ds(pl.multiple_of(slot * rows, rows), rows), :]

    def ag(slot, device, k, part, recv):
        piece = xbuf.at[
            pl.ds(pl.multiple_of(slot * rows, rows), rows), part * wide : (part + 1) * wide
        ]
        return remote(piece, piece, ag_s.at[k], recv, device)

    def ag_near(slot, device, k, part):
        return ag(slot, device, k, part, ag_r.at[slot // 2, part])

    def ag_over(slot, k, part):
        return ag(slot, partner, k, part, ag_p.at[slot // 2])

    parts_x = range(PIECES)
    for q in parts_x:
        ag_near(tp, fwd, 0, q).start()
    for q in parts_x:
        ag_over(tp, 1, q).start()
    all_sent(block(tp), ag_s.at[0])
    for q in parts_x:
        ag_near(tp, bwd, 2, q).start()
    for q in parts_x:
        ag_near(2 * x_bwd + c, fwd, 3, q).wait_recv()
        ag_near(2 * x_bwd + c, fwd, 3, q).start()
    for q in parts_x:
        ag_over(2 * x_bwd + c, 4, q).start()
    for slot, k in ((2 * x_fwd + c, 5), (2 * x_far + c, 6)):
        for q in parts_x:
            ag_near(slot, fwd, k, q).wait_recv()
            ag_over(slot, k, q).start()
    for i in range(X):
        all_here(block(2 * i + 1 - c), ag_p.at[i])

    per = max(H // 2, 1)
    tall = WIDTH // per

    def weights(slot, device, k, q):
        at = pl.multiple_of(slot * WIDTH + q % per * tall, tall)
        piece = wfull.at[q // per, pl.ds(at, tall), :]
        recv = wg_r.at[slot // 2, q] if k in (0, 1, 3) else wg_p.at[q // per, slot // 2]
        return remote(piece, piece, wg_s.at[k], recv, device)

    def own_weights(q):
        weights(tp, fwd, 0, q).start()
        weights(tp, bwd, 1, q).start()
        weights(tp, partner, 2, q).start()

    def weights_step(s):
        @pl.when(jnp.logical_and(s >= 2, s - 2 < H))
        def _():
            q = s - 2
            turn = way * (1 - 2 * (q % 2))
            src, dst = (x - turn + X) % X, (x + turn + X) % X
            weights(2 * src + c, fwd, 3, q).wait_recv()
            weights(2 * src + c, (sp, 2 * dst + c), 3, q).start()
            weights(2 * src + c, partner, 4, q).start()
            weights(2 * dst + c, fwd, 3, q).wait_recv()
            weights(2 * dst + c, partner, 5, q).start()

        @pl.when(s + 1 < H)
        def _():
            own_weights(s + 1)

        @pl.when(jnp.logical_and(s >= 4, s - 4 < H))
        def _():
            weights(2 * x_far + c, fwd, 3, s - 4).wait_recv()
            weights(2 * x_far + c, partner, 6, s - 4).start()

    def weights_here(kind):
        for i in range(X):
            at = pl.multiple_of((2 * i + 1 - c) * WIDTH, WIDTH)
            all_here(wfull.at[kind, pl.ds(at, WIDTH), :], wg_p.at[kind, i])

    for load in loads[:2]:
        load.wait()
    normed = xbuf[...]
    kv = jnp.dot(normed, wcat[:, : 2 * WIDTH], preferred_element_type=F32)
    kbuf[z] = kv[:, :WIDTH].astype(BF16)
    vbuf[z] = kv[:, WIDTH:].T.astype(BF16)

    bufs = (kbuf, vbuf)

    def ring(way_, kind, slot, step):
        half = bufs[kind // HALVES].shape[1] // HALVES
        at = kind % HALVES * half
        piece = bufs[kind // HALVES].at[slot, at : at + half, :]
        return remote(
            piece, piece, kv_s.at[way_, kind // HALVES], kv_r.at[kind, slot], (z_up, z_down)[way_]
        )

    kinds = list(range(2 * HALVES))
    for kind in kinds:
        ring(0, kind, z, 0).start()
        if G > 0:
            ring(1, kind, z, 0).start()

    for load in loads[2:4]:
        load.wait()
    qg = jnp.dot(normed, wcat[:, 2 * WIDTH : 4 * WIDTH], preferred_element_type=F32)
    qbuf[y] = qg[:, :WIDTH].T.astype(BF16)
    for d in range(1, Y):
        remote(qbuf.at[y], qbuf.at[y], q_s, q_r, plane(d)).start()
    gate_s[...] = qg[:, WIDTH:].astype(BF16)

    for load in loads[4:]:
        load.wait()
    for q in range(min(2, H)):
        own_weights(q)
    rr = jnp.dot(normed, wcat[:, 4 * WIDTH :], preferred_element_type=F32)
    rec_s[...] = rr[:, :WIDTH].astype(BF16)
    remote(rec_s.at[R - 16 :, :], halo, halo_s, halo_r, sp_next).start()
    recg_s[...] = rr[:, WIDTH:].astype(BF16)


    sub = lax.broadcasted_iota(jnp.int32, (8, WIDTH), 0)

    def block_scan():
        row = lax.broadcasted_iota(jnp.int32, (R, WIDTH), 0)
        remote(halo, halo, halo_s, halo_r, sp_next).wait_recv()
        ext[0:16, :] = jnp.where(sp > 0, halo[...].astype(F32), 0.0)
        ext[16:, :] = rec_s[...].astype(F32)
        conv = jnp.zeros((R, WIDTH), F32)
        for j in range(4):
            conv = conv + ext[13 + j : 13 + j + R, :] * conv_taps[j : j + 1, :]
        conv_out = conv.astype(BF16)
        recur = jax.nn.sigmoid(jnp.dot(conv_out, gate_recur[0], preferred_element_type=F32))
        inflow = jax.nn.sigmoid(jnp.dot(conv_out, gate_input[0], preferred_element_type=F32))
        log_decay = -RATE_SCALE * recur * decay_rate[...]
        first = jnp.logical_and(row == 0, sp == 0)
        factor = jnp.where(first, 1.0, jnp.sqrt(minus_expm1(2.0 * log_decay)))
        a = jnp.exp(log_decay)
        b = factor * inflow * conv_out.astype(F32)
        k = 1
        while k < R:
            inside = row >= k
            b = b + a * jnp.where(inside, pltpu.roll(b, k, 0), 0.0)
            a = a * jnp.where(inside, pltpu.roll(a, k, 0), 1.0)
            k *= 2
        prods[...] = a
        parts[...] = b
        yagg[y] = jnp.where(sub == 0, a[R - 1 : R, :], b[R - 1 : R, :])
        for d in range(1, Y):
            agg_copy(d).start()
        return

    def agg_copy(d):
        return remote(yagg.at[y], yagg.at[y], ya_s, ya_r, plane(d))

    def plane_total():
        all_here(yagg.at[0 : Y - 1], ya_r)
        ta, tb = yagg[0, 0:1, :], yagg[0, 1:2, :]
        for i in range(1, Y):
            ia, ib = yagg[i, 0:1, :], yagg[i, 1:2, :]
            ta, tb = ia * ta, ia * tb + ib
        zagg[z] = jnp.where(sub == 0, ta, tb)
        state(0, z, 0).start()
        if G > 0:
            state(1, z, 0).start()

    def state(way_, slot, step):
        piece = zagg.at[slot]
        return remote(piece, piece, za_s.at[way_], za_r.at[slot], (z_up, z_down)[way_])

    def state_step(j):
        up, down = (z - j + Z) % Z, (z + j) % Z
        state(0, up, 0).wait_recv()

        @pl.when(j < H)
        def _():
            state(0, up, j).start()

        @pl.when(j <= G)
        def _():
            state(1, down, 0).wait_recv()

            @pl.when(j < G)
            def _():
                state(1, down, j).start()

    def tile(slot, opening):
        key = kbuf[slot]
        keys = jnp.concatenate([key, key], axis=1)
        value = vbuf[slot]
        n = 2 * Y
        score = lambda i: jnp.dot(keys, qext[i], preferred_element_type=F32)
        scores = [score(i) for i in range(n)]

        for i in range(n):
            s = scores[i]
            if opening:
                pos = lax.broadcasted_iota(jnp.int32, (R, R), 1) - lax.broadcasted_iota(
                    jnp.int32, (R, R), 0
                )
                allowed = pos + (i // 2 - y) * R >= 0
                s = jnp.where(allowed, s, MASKED)
                top = jnp.max(s, axis=0, keepdims=True)
                p = jnp.where(allowed, jnp.exp2(s - top), 0.0)
                l_ref[i : i + 1, :] = jnp.sum(p, axis=0, keepdims=True)
                acc[i] = jnp.dot(value, p.astype(BF16), preferred_element_type=F32)
            else:
                old = m_ref[i : i + 1, :]
                top = jnp.maximum(old, jnp.max(s, axis=0, keepdims=True))
                p = jnp.exp2(s - top)
                fade = jnp.exp2(old - top)
                l_ref[i : i + 1, :] = l_ref[i : i + 1, :] * fade + jnp.sum(p, axis=0, keepdims=True)
                acc[i] = acc[i] * fade + jnp.dot(value, p.astype(BF16), preferred_element_type=F32)
            m_ref[i : i + 1, :] = top

    def last_scores(slot):
        key = kbuf[slot]
        keys = jnp.concatenate([key, key], axis=1)
        scores = [jnp.dot(keys, qext[i], preferred_element_type=F32) for i in range(2 * Y)]
        for i in range(2 * Y):
            old = m_ref[i : i + 1, :]
            top = jnp.maximum(old, jnp.max(scores[i], axis=0, keepdims=True))
            p = jnp.exp2(scores[i] - top)
            fade = jnp.exp2(old - top)
            l_ref[i : i + 1, :] = l_ref[i : i + 1, :] * fade + jnp.sum(p, axis=0, keepdims=True)
            last_p[i] = p.astype(BF16)
            last_f[i : i + 1, :] = fade
            m_ref[i : i + 1, :] = top

    def last_values(slot):
        value = vbuf[slot]
        for i in range(2 * Y):
            acc[i] = acc[i] * last_f[i : i + 1, :] + jnp.dot(
                value, last_p[i], preferred_element_type=F32
            )

    def opening():
        all_here(qbuf.at[0 : Y - 1], q_r)
        half = WIDTH // 2
        none = jnp.zeros((half, R), BF16)
        for i in range(Y):
            q = qbuf[i].astype(F32) * (LOG2E * half ** -0.5)
            high = q.astype(BF16)
            low = (q - high.astype(F32)).astype(BF16)
            qext[2 * i] = jnp.concatenate([high[:half], none, low[:half], none], axis=0)
            qext[2 * i + 1] = jnp.concatenate([none, high[half:], none, low[half:]], axis=0)
        tile(z, True)

    def pass_on(s, some):
        up, down = (z - s + Z) % Z, (z + s) % Z
        for kind in some:
            ring(0, kind, up, 0).wait_recv()

            @pl.when(s < H)
            def _():
                ring(0, kind, up, s).start()

            @pl.when(s <= G)
            def _():
                ring(1, kind, down, 0).wait_recv()

                @pl.when(s < G)
                def _():
                    ring(1, kind, down, s).start()

    def step(s, carry):
        pass_on(s, kinds[:HALVES])

        @pl.when(s == 1)
        def _():
            block_scan()

        @pl.when(jnp.logical_and(s > 1, z >= s - 1))
        def _():
            tile((z - s + 1 + Z) % Z, False)

        @pl.when(s < H)
        def _():
            pass_on(s, kinds[HALVES:])

        @pl.when(s == 1)
        def _():
            opening()

        @pl.when(jnp.logical_and(s > 1, z + s - 1 >= Z))
        def _():
            tile((z + s - 1) % Z, False)

        @pl.when(s == 2)
        def _():
            plane_total()

        @pl.when(s > 2)
        def _():
            state_step(s - 2)

        weights_step(s)
        return carry

    lax.fori_loop(1, H + 1, step, 0)

    @pl.when(z >= H)
    def _():
        last_scores(z - H)

    stat[y, 0 : 2 * Y, :] = m_ref[0 : 2 * Y, :]
    stat[y, 2 * Y : 4 * Y, :] = l_ref[0 : 2 * Y, :]
    for d in range(1, Y):
        remote(stat.at[y], stat.at[y], st_s, st_r, plane(d)).start()
    pass_on(jnp.int32(H), kinds[HALVES:])

    @pl.when(z >= H)
    def _():
        last_values(z - H)

    all_here(stat.at[0 : Y - 1], st_r)
    lam = head_lambda[...]

    def comb_copy(i):
        return remote(cbuf.at[i], pbuf.at[y], cb_s, cb_r, (z * Y + i, tp))

    for i in range(Y):
        weight = []
        for n in (2 * i, 2 * i + 1):
            tops = [stat[j, n : n + 1, :] for j in range(Y)]
            top = functools.reduce(jnp.maximum, tops)
            total = sum(stat[j, 2 * Y + n : 2 * Y + n + 1, :] * jnp.exp2(tops[j] - top) for j in range(Y))
            weight.append(jnp.exp2(m_ref[n : n + 1, :] - top) / total)
        comb = acc[2 * i] * weight[0] - acc[2 * i + 1] * (weight[1] * lam)

        @pl.when(y == i)
        def _():
            own_c[...] = comb

        @pl.when(y != i)
        def _():
            cbuf[i] = comb.astype(BF16)
            comb_copy(i).start()

    weights_step(jnp.int32(H + 1))
    if H > 1:
        state_step(H - 1)
    state_step(H)

    h = jnp.zeros((1, WIDTH), F32)
    for i in range(Z - 1):
        h = jnp.where(i < z, zagg[i, 0:1, :] * h + zagg[i, 1:2, :], h)
    for i in range(Y - 1):
        h = jnp.where(i < y, yagg[i, 0:1, :] * h + yagg[i, 1:2, :], h)
    states = parts[...] + prods[...] * h
    recg = recg_s[...].astype(F32)
    rec_m[...] = (states * (recg * jax.nn.sigmoid(recg))).astype(BF16)

    def share(mine, theirs, ss, rs, d):
        peer = (tp + d) % (2 * X)
        piece = mine.at[pl.ds(pl.multiple_of(peer * rows, rows), rows), :]
        return remote(piece, theirs.at[tp], ss, rs, row_peer(d))

    def shared(mine, theirs, ss, rs):
        all_here(theirs.at[0 : 2 * X - 1], rs)
        theirs[tp] = mine[pl.ds(pl.multiple_of(tp * rows, rows), rows), :]
        return jnp.concatenate([theirs[i] for i in range(2 * X)], axis=1)

    for way_, count in ((0, H), (1, G)):
        if count > 0:
            all_sent(kbuf.at[0:count], kv_s.at[way_, 0])
            all_sent(vbuf.at[0:count], kv_s.at[way_, 1])
            all_sent(zagg.at[0:count], za_s.at[way_])
    if Y > 1:
        all_sent(yagg.at[0 : Y - 1], ya_s)
        all_sent(qbuf.at[0 : Y - 1], q_s)
        all_sent(stat.at[0 : Y - 1], st_s)
    all_sent(halo, halo_s)
    weights_step(jnp.int32(H + 2))
    for d in range(1, 2 * X):
        share(rec_m, rec_g, rm_s, rm_r, d).start()
    total = own_c[...]
    all_here(pbuf.at[0 : Y - 1], cb_r)
    for d in range(1, Y):
        total = total + pbuf[(y + d) % Y].astype(F32)
    total = total * lax.rsqrt(jnp.mean(total * total, axis=0, keepdims=True) + EPS_HEAD)
    gate = gate_s[...].astype(F32)
    att = total.T * head_gain[...] * HEAD_FACTOR * (gate * jax.nn.sigmoid(gate))
    att_m[...] = att.astype(BF16)
    for d in range(1, 2 * X):
        share(att_m, att_g, am_s, am_r, d).start()

    weights_step(jnp.int32(H + 3))

    mine = pl.ds(pl.multiple_of(tp * WIDTH, WIDTH), WIDTH)
    for k in range(7):
        all_sent(wfull.at[:, mine, :], wg_s.at[k])
    for k in range(1, 7):
        all_sent(block(tp), ag_s.at[k])
    all_sent(pbuf.at[0 : Y - 1], cb_s)
    all_sent(rec_m.at[0 : (2 * X - 1) * rows, :], rm_s)
    weights_here(0)
    left = shared(rec_m, rec_g, rm_s, rm_r)
    for q in parts_x:
        cols = slice(q * wide, (q + 1) * wide)
        out_a[:, cols] = jnp.dot(left, wfull[0, :, cols], preferred_element_type=F32)
    if H > 1:
        weights_here(1)
    left = shared(att_m, att_g, am_s, am_r)
    for q in parts_x:
        cols = slice(q * wide, (q + 1) * wide)
        part = jnp.dot(left, wfull[1, :, cols], preferred_element_type=F32)
        out[:, cols] = (out_a[:, cols] + part).astype(BF16)

    all_sent(att_m.at[0 : (2 * X - 1) * rows, :], am_s)


def build(mesh, Y):
    SP, TP = mesh.shape["sp"], mesh.shape["tp"]
    Z, X = SP // Y, TP // 2

    def body(
        tokens, norm_gain, w_query, w_key, w_value, w_att_gate, w_rec_in, w_rec_gate, conv_taps,
        gate_recur, gate_input, decay_rate, head_lambda, head_gain, out_att, out_rec,
    ):
        rows, D = tokens.shape
        R = rows * TP
        H, G = Z // 2, max(Z - 1 - Z // 2, 1)
        vmem, far = pl.BlockSpec(memory_space=pltpu.VMEM), pl.BlockSpec(memory_space=pl.ANY)
        V, dma = pltpu.VMEM, pltpu.SemaphoreType.DMA
        scratch = [
            V((D, 6 * WIDTH), BF16), V((2, TP * WIDTH, D), BF16), V((R, D), BF16),
            V((Z, R, WIDTH), BF16), V((Z, WIDTH, R), BF16), V((Y, WIDTH, R), BF16),
            V((2 * Y, 2 * WIDTH, R), BF16), V((2 * Y, WIDTH, R), F32),
            V((2 * Y, R), F32), V((2 * Y, R), F32), V((2 * Y, R, R), BF16), V((2 * Y, R), F32),
            V((R, WIDTH), BF16), V((R, WIDTH), BF16), V((R, WIDTH), BF16),
            V((16, WIDTH), BF16), V((R + 16, WIDTH), F32),
            V((R, WIDTH), F32), V((R, WIDTH), F32), V((Y, 8, WIDTH), F32), V((Z, 8, WIDTH), F32),
            V((Y, 4 * Y, R), F32), V((Y, WIDTH, R), BF16), V((Y, WIDTH, R), BF16),
            V((WIDTH, R), F32), V((R, WIDTH), BF16), V((R, WIDTH), BF16),
            V((TP, rows, WIDTH), BF16), V((TP, rows, WIDTH), BF16), V((rows, D), F32),
            dma((8,)), dma((7,)), dma((X, PIECES)), dma((X,)), dma((2, 2)), dma((2 * HALVES, Z)),
            dma(()), dma(()), dma(()), dma(()), dma(()), dma(()), dma((2,)), dma((Z,)),
            dma(()), dma(()), dma(()), dma(()), dma((7,)), dma((X, H)), dma((2, X)),
            dma(()), dma(()), dma(()), dma(()),
        ]
        return pl.pallas_call(
            functools.partial(kernel, Z, Y, X),
            out_shape=jax.ShapeDtypeStruct((rows, D), BF16),
            in_specs=[vmem, vmem] + [far] * 6 + [vmem] * 6 + [far] * 2,
            out_specs=vmem,
            scratch_shapes=scratch,
            compiler_params=pltpu.CompilerParams(
                collective_id=0, has_side_effects=True, vmem_limit_bytes=56 * 1024 * 1024
            ),
        )(
            tokens, norm_gain.reshape(1, -1), w_query, w_key, w_value, w_att_gate, w_rec_in,
            w_rec_gate, conv_taps, gate_recur, gate_input, decay_rate.reshape(1, -1),
            head_lambda.reshape(1, 1), head_gain.reshape(1, -1), out_att, out_rec,
        )

    both = P(("sp", "tp"), None)
    cols, lead = P(None, "tp"), P("tp")
    placed = (
        both, P(), cols, cols, cols, cols, cols, cols, cols,
        P("tp", None, None), P("tp", None, None), lead, lead, lead, P("tp", None), P("tp", None),
    )
    return jax.shard_map(body, mesh=mesh, in_specs=placed, out_specs=both, check_vma=False)


def solution(mesh):
    return build(mesh, 4)
```

```python
import functools
import math

import jax
import jax.numpy as jnp
from jax import lax
from jax.experimental import pallas as pl
from jax.experimental.pallas import tpu as pltpu
from jax.sharding import PartitionSpec as P

MESH = pl.DeviceIdType.MESH
F32 = jnp.float32
BF16 = jnp.bfloat16

EPS_INPUT = 1e-06
EPS_HEAD = 1e-05
RATE_SCALE = 8.0
HEAD_FACTOR = 0.8
MASKED = -1e30
LOG2E = math.log2(math.e)
PIECES = 4
HALVES = 2
WIDTH = 128


def minus_expm1(x):
    series = 1.0 + x * (
        1 / 2 + x * (1 / 6 + x * (1 / 24 + x * (1 / 120 + x * (1 / 720 + x * (1 / 5040)))))
    )
    return jnp.where(x > -0.5, -x * series, 1.0 - jnp.exp(x))


def kernel(
    Z, Y, X,
    tokens, norm_gain, w_query, w_key, w_value, w_att_gate, w_rec_in, w_rec_gate, conv_taps,
    gate_recur, gate_input, decay_rate, head_lambda, head_gain, out_att, out_rec,
    out,
    wcat, wfull, xbuf, kbuf, vbuf, qbuf, qext, acc, m_ref, l_ref, last_p, last_f, gate_s, rec_s, recg_s, halo, ext,
    prods, parts, yagg, zagg, stat, cbuf, pbuf, own_c, att_m, rec_m, att_g, rec_g, out_a,
    w_sem, ag_s, ag_r, ag_p, kv_s, kv_r, q_s, q_r, halo_s, halo_r, ya_s, ya_r, za_s, za_r,
    st_s, st_r, cb_s, cb_r, wg_s, wg_r, wg_p, am_s, am_r, rm_s, rm_r,
):
    rows = tokens.shape[0]
    R = xbuf.shape[0]
    H, G = Z // 2, Z - 1 - Z // 2
    wide = tokens.shape[1] // PIECES
    sp, tp = lax.axis_index("sp"), lax.axis_index("tp")
    z, y = sp // Y, sp % Y
    x, c = tp // 2, tp % 2
    way = 1 - 2 * c
    x_fwd, x_bwd, x_far = (x + way + X) % X, (x - way + X) % X, (x + 2) % X
    partner = (sp, 2 * x + 1 - c)
    fwd, bwd = (sp, 2 * x_fwd + c), (sp, 2 * x_bwd + c)
    z_up, z_down = (((z + 1) % Z) * Y + y, tp), (((z + Z - 1) % Z) * Y + y, tp)
    sp_next, sp_prev = ((sp + 1) % (Z * Y), tp), ((sp + Z * Y - 1) % (Z * Y), tp)

    def plane(d):
        return (z * Y + (y + d) % Y, tp)

    def row_peer(d):
        return (sp, (tp + d) % (2 * X))

    def remote(src, dst, send, recv, device):
        return pltpu.make_async_remote_copy(
            src_ref=src, dst_ref=dst, send_sem=send, recv_sem=recv,
            device_id=device, device_id_type=MESH,
        )

    def all_sent(piece, sem):
        remote(piece, piece, sem, sem, partner).wait_send()

    def all_here(piece, sem):
        remote(piece, piece, sem, sem, partner).wait_recv()

    loads = [
        pltpu.make_async_copy(w, wcat.at[:, i * WIDTH : (i + 1) * WIDTH], w_sem.at[i])
        for i, w in enumerate((w_key, w_value, w_query, w_att_gate, w_rec_in, w_rec_gate))
    ]
    loads += [
        pltpu.make_async_copy(
            w, wfull.at[i, pl.ds(pl.multiple_of(tp * WIDTH, WIDTH), WIDTH), :], w_sem.at[6 + i]
        )
        for i, w in enumerate((out_rec, out_att))
    ]
    for load in loads:
        load.start()

    barrier = pltpu.get_barrier_semaphore()
    peers = [z_up, z_down, sp_next, sp_prev] + [plane(d) for d in range(1, Y)]
    peers += [row_peer(d) for d in range(1, 2 * X)]
    for peer in peers:
        pl.semaphore_signal(barrier, inc=1, device_id=peer, device_id_type=MESH)

    tok = tokens[...].astype(F32)
    scale = lax.rsqrt(jnp.mean(tok * tok, axis=-1, keepdims=True) + EPS_INPUT)
    xbuf[pl.ds(pl.multiple_of(tp * rows, rows), rows), :] = (tok * scale * norm_gain[...]).astype(BF16)

    pl.semaphore_wait(barrier, len(peers))

    def block(slot):
        return xbuf.at[pl.ds(pl.multiple_of(slot * rows, rows), rows), :]

    def ag(slot, device, k, part, recv):
        piece = xbuf.at[
            pl.ds(pl.multiple_of(slot * rows, rows), rows), part * wide : (part + 1) * wide
        ]
        return remote(piece, piece, ag_s.at[k], recv, device)

    def ag_near(slot, device, k, part):
        return ag(slot, device, k, part, ag_r.at[slot // 2, part])

    def ag_over(slot, k, part):
        return ag(slot, partner, k, part, ag_p.at[slot // 2])

    parts_x = range(PIECES)
    for q in parts_x:
        ag_near(tp, fwd, 0, q).start()
    for q in parts_x:
        ag_over(tp, 1, q).start()
    all_sent(block(tp), ag_s.at[0])
    for q in parts_x:
        ag_near(tp, bwd, 2, q).start()
    for q in parts_x:
        ag_near(2 * x_bwd + c, fwd, 3, q).wait_recv()
        ag_near(2 * x_bwd + c, fwd, 3, q).start()
    for q in parts_x:
        ag_over(2 * x_bwd + c, 4, q).start()
    for slot, k in ((2 * x_fwd + c, 5), (2 * x_far + c, 6)):
        for q in parts_x:
            ag_near(slot, fwd, k, q).wait_recv()
            ag_over(slot, k, q).start()
    for i in range(X):
        all_here(block(2 * i + 1 - c), ag_p.at[i])

    per = max(H // 2, 1)
    tall = WIDTH // per

    def weights(slot, device, k, q):
        at = pl.multiple_of(slot * WIDTH + q % per * tall, tall)
        piece = wfull.at[q // per, pl.ds(at, tall), :]
        recv = wg_r.at[slot // 2, q] if k in (0, 1, 3) else wg_p.at[q // per, slot // 2]
        return remote(piece, piece, wg_s.at[k], recv, device)

    def own_weights(q):
        weights(tp, fwd, 0, q).start()
        weights(tp, bwd, 1, q).start()
        weights(tp, partner, 2, q).start()

    def weights_step(s):
        @pl.when(jnp.logical_and(s >= 2, s - 2 < H))
        def _():
            q = s - 2
            turn = way * (1 - 2 * (q % 2))
            src, dst = (x - turn + X) % X, (x + turn + X) % X
            weights(2 * src + c, fwd, 3, q).wait_recv()
            weights(2 * src + c, (sp, 2 * dst + c), 3, q).start()
            weights(2 * src + c, partner, 4, q).start()
            weights(2 * dst + c, fwd, 3, q).wait_recv()
            weights(2 * dst + c, partner, 5, q).start()

        @pl.when(s + 1 < H)
        def _():
            own_weights(s + 1)

        @pl.when(jnp.logical_and(s >= 4, s - 4 < H))
        def _():
            weights(2 * x_far + c, fwd, 3, s - 4).wait_recv()
            weights(2 * x_far + c, partner, 6, s - 4).start()

    def weights_here(kind):
        for i in range(X):
            at = pl.multiple_of((2 * i + 1 - c) * WIDTH, WIDTH)
            all_here(wfull.at[kind, pl.ds(at, WIDTH), :], wg_p.at[kind, i])

    for load in loads[:2]:
        load.wait()
    normed = xbuf[...]
    kv = jnp.dot(normed, wcat[:, : 2 * WIDTH], preferred_element_type=F32)
    kbuf[z] = kv[:, :WIDTH].astype(BF16)
    vbuf[z] = kv[:, WIDTH:].T.astype(BF16)

    bufs = (kbuf, vbuf)

    def ring(way_, kind, slot, step):
        half = bufs[kind // HALVES].shape[1] // HALVES
        at = kind % HALVES * half
        piece = bufs[kind // HALVES].at[slot, at : at + half, :]
        return remote(
            piece, piece, kv_s.at[way_, kind // HALVES], kv_r.at[kind, slot], (z_up, z_down)[way_]
        )

    kinds = list(range(2 * HALVES))
    for kind in kinds:
        ring(0, kind, z, 0).start()
        if G > 0:
            ring(1, kind, z, 0).start()

    for load in loads[2:4]:
        load.wait()
    qg = jnp.dot(normed, wcat[:, 2 * WIDTH : 4 * WIDTH], preferred_element_type=F32)
    qbuf[y] = qg[:, :WIDTH].T.astype(BF16)
    for d in range(1, Y):
        remote(qbuf.at[y], qbuf.at[y], q_s, q_r, plane(d)).start()
    gate_s[...] = qg[:, WIDTH:].astype(BF16)

    for load in loads[4:]:
        load.wait()
    for q in range(min(2, H)):
        own_weights(q)
    rr = jnp.dot(normed, wcat[:, 4 * WIDTH :], preferred_element_type=F32)
    rec_s[...] = rr[:, :WIDTH].astype(BF16)
    remote(rec_s.at[R - 16 :, :], halo, halo_s, halo_r, sp_next).start()
    recg_s[...] = rr[:, WIDTH:].astype(BF16)


    sub = lax.broadcasted_iota(jnp.int32, (8, WIDTH), 0)

    def block_scan():
        row = lax.broadcasted_iota(jnp.int32, (R, WIDTH), 0)
        remote(halo, halo, halo_s, halo_r, sp_next).wait_recv()
        ext[0:16, :] = jnp.where(sp > 0, halo[...].astype(F32), 0.0)
        ext[16:, :] = rec_s[...].astype(F32)
        conv = jnp.zeros((R, WIDTH), F32)
        for j in range(4):
            conv = conv + ext[13 + j : 13 + j + R, :] * conv_taps[j : j + 1, :]
        conv_out = conv.astype(BF16)
        recur = jax.nn.sigmoid(jnp.dot(conv_out, gate_recur[0], preferred_element_type=F32))
        inflow = jax.nn.sigmoid(jnp.dot(conv_out, gate_input[0], preferred_element_type=F32))
        log_decay = -RATE_SCALE * recur * decay_rate[...]
        first = jnp.logical_and(row == 0, sp == 0)
        factor = jnp.where(first, 1.0, jnp.sqrt(minus_expm1(2.0 * log_decay)))
        a = jnp.exp(log_decay)
        b = factor * inflow * conv_out.astype(F32)
        k = 1
        while k < R:
            inside = row >= k
            b = b + a * jnp.where(inside, pltpu.roll(b, k, 0), 0.0)
            a = a * jnp.where(inside, pltpu.roll(a, k, 0), 1.0)
            k *= 2
        prods[...] = a
        parts[...] = b
        yagg[y] = jnp.where(sub == 0, a[R - 1 : R, :], b[R - 1 : R, :])
        for d in range(1, Y):
            agg_copy(d).start()
        return

    def agg_copy(d):
        return remote(yagg.at[y], yagg.at[y], ya_s, ya_r, plane(d))

    def plane_total():
        all_here(yagg.at[0 : Y - 1], ya_r)
        ta, tb = yagg[0, 0:1, :], yagg[0, 1:2, :]
        for i in range(1, Y):
            ia, ib = yagg[i, 0:1, :], yagg[i, 1:2, :]
            ta, tb = ia * ta, ia * tb + ib
        zagg[z] = jnp.where(sub == 0, ta, tb)
        state(0, z, 0).start()
        if G > 0:
            state(1, z, 0).start()

    def state(way_, slot, step):
        piece = zagg.at[slot]
        return remote(piece, piece, za_s.at[way_], za_r.at[slot], (z_up, z_down)[way_])

    def state_step(j):
        up, down = (z - j + Z) % Z, (z + j) % Z
        state(0, up, 0).wait_recv()

        @pl.when(j < H)
        def _():
            state(0, up, j).start()

        @pl.when(j <= G)
        def _():
            state(1, down, 0).wait_recv()

            @pl.when(j < G)
            def _():
                state(1, down, j).start()

    def tile(slot, opening):
        key = kbuf[slot]
        keys = jnp.concatenate([key, key], axis=1)
        value = vbuf[slot]
        n = 2 * Y
        score = lambda i: jnp.dot(keys, qext[i], preferred_element_type=F32)
        scores = [score(i) for i in range(n)]

        for i in range(n):
            s = scores[i]
            if opening:
                pos = lax.broadcasted_iota(jnp.int32, (R, R), 1) - lax.broadcasted_iota(
                    jnp.int32, (R, R), 0
                )
                allowed = pos + (i // 2 - y) * R >= 0
                s = jnp.where(allowed, s, MASKED)
                top = jnp.max(s, axis=0, keepdims=True)
                p = jnp.where(allowed, jnp.exp2(s - top), 0.0)
                l_ref[i : i + 1, :] = jnp.sum(p, axis=0, keepdims=True)
                acc[i] = jnp.dot(value, p.astype(BF16), preferred_element_type=F32)
            else:
                old = m_ref[i : i + 1, :]
                top = jnp.maximum(old, jnp.max(s, axis=0, keepdims=True))
                p = jnp.exp2(s - top)
                fade = jnp.exp2(old - top)
                l_ref[i : i + 1, :] = l_ref[i : i + 1, :] * fade + jnp.sum(p, axis=0, keepdims=True)
                acc[i] = acc[i] * fade + jnp.dot(value, p.astype(BF16), preferred_element_type=F32)
            m_ref[i : i + 1, :] = top

    def last_scores(slot):
        key = kbuf[slot]
        keys = jnp.concatenate([key, key], axis=1)
        scores = [jnp.dot(keys, qext[i], preferred_element_type=F32) for i in range(2 * Y)]
        for i in range(2 * Y):
            old = m_ref[i : i + 1, :]
            top = jnp.maximum(old, jnp.max(scores[i], axis=0, keepdims=True))
            p = jnp.exp2(scores[i] - top)
            fade = jnp.exp2(old - top)
            l_ref[i : i + 1, :] = l_ref[i : i + 1, :] * fade + jnp.sum(p, axis=0, keepdims=True)
            last_p[i] = p.astype(BF16)
            last_f[i : i + 1, :] = fade
            m_ref[i : i + 1, :] = top

    def last_values(slot):
        value = vbuf[slot]
        for i in range(2 * Y):
            acc[i] = acc[i] * last_f[i : i + 1, :] + jnp.dot(
                value, last_p[i], preferred_element_type=F32
            )

    def opening():
        all_here(qbuf.at[0 : Y - 1], q_r)
        half = WIDTH // 2
        none = jnp.zeros((half, R), BF16)
        for i in range(Y):
            q = qbuf[i].astype(F32) * (LOG2E * half ** -0.5)
            high = q.astype(BF16)
            low = (q - high.astype(F32)).astype(BF16)
            qext[2 * i] = jnp.concatenate([high[:half], none, low[:half], none], axis=0)
            qext[2 * i + 1] = jnp.concatenate([none, high[half:], none, low[half:]], axis=0)
        tile(z, True)

    def pass_on(s, some):
        up, down = (z - s + Z) % Z, (z + s) % Z
        for kind in some:
            ring(0, kind, up, 0).wait_recv()

            @pl.when(s < H)
            def _():
                ring(0, kind, up, s).start()

            @pl.when(s <= G)
            def _():
                ring(1, kind, down, 0).wait_recv()

                @pl.when(s < G)
                def _():
                    ring(1, kind, down, s).start()

    def step(s, carry):
        pass_on(s, kinds[:HALVES])

        @pl.when(s == 1)
        def _():
            block_scan()

        @pl.when(jnp.logical_and(s > 1, z >= s - 1))
        def _():
            tile((z - s + 1 + Z) % Z, False)

        @pl.when(s < H)
        def _():
            pass_on(s, kinds[HALVES:])

        @pl.when(s == 1)
        def _():
            opening()

        @pl.when(jnp.logical_and(s > 1, z + s - 1 >= Z))
        def _():
            tile((z + s - 1) % Z, False)

        @pl.when(s == 2)
        def _():
            plane_total()

        @pl.when(s > 2)
        def _():
            state_step(s - 2)

        weights_step(s)
        return carry

    lax.fori_loop(1, H + 1, step, 0)

    @pl.when(z >= H)
    def _():
        last_scores(z - H)

    stat[y, 0 : 2 * Y, :] = m_ref[0 : 2 * Y, :]
    stat[y, 2 * Y : 4 * Y, :] = l_ref[0 : 2 * Y, :]
    for d in range(1, Y):
        remote(stat.at[y], stat.at[y], st_s, st_r, plane(d)).start()
    pass_on(jnp.int32(H), kinds[HALVES:])

    @pl.when(z >= H)
    def _():
        last_values(z - H)

    weights_step(jnp.int32(H + 1))
    if H > 1:
        state_step(H - 1)
    all_here(stat.at[0 : Y - 1], st_r)
    lam = head_lambda[...]

    def comb_copy(i):
        return remote(cbuf.at[i], pbuf.at[y], cb_s, cb_r, (z * Y + i, tp))

    for i in range(Y):
        weight = []
        for n in (2 * i, 2 * i + 1):
            tops = [stat[j, n : n + 1, :] for j in range(Y)]
            top = functools.reduce(jnp.maximum, tops)
            total = sum(stat[j, 2 * Y + n : 2 * Y + n + 1, :] * jnp.exp2(tops[j] - top) for j in range(Y))
            weight.append(jnp.exp2(m_ref[n : n + 1, :] - top) / total)
        comb = acc[2 * i] * weight[0] - acc[2 * i + 1] * (weight[1] * lam)

        @pl.when(y == i)
        def _():
            own_c[...] = comb

        cbuf[i] = comb.astype(BF16)

    for d in sorted(range(1, Y), key=lambda d: -min(d, Y - d)):
        comb_copy((y + d) % Y).start()

    state_step(H)

    h = jnp.zeros((1, WIDTH), F32)
    for i in range(Z - 1):
        h = jnp.where(i < z, zagg[i, 0:1, :] * h + zagg[i, 1:2, :], h)
    for i in range(Y - 1):
        h = jnp.where(i < y, yagg[i, 0:1, :] * h + yagg[i, 1:2, :], h)
    states = parts[...] + prods[...] * h
    recg = recg_s[...].astype(F32)
    rec_m[...] = (states * (recg * jax.nn.sigmoid(recg))).astype(BF16)

    def share(mine, theirs, ss, rs, d):
        peer = (tp + d) % (2 * X)
        piece = mine.at[pl.ds(pl.multiple_of(peer * rows, rows), rows), :]
        return remote(piece, theirs.at[tp], ss, rs, row_peer(d))

    def shared(mine, theirs, ss, rs):
        all_here(theirs.at[0 : 2 * X - 1], rs)
        theirs[tp] = mine[pl.ds(pl.multiple_of(tp * rows, rows), rows), :]
        return jnp.concatenate([theirs[i] for i in range(2 * X)], axis=1)

    for d in range(1, 2 * X):
        share(rec_m, rec_g, rm_s, rm_r, d).start()
    for way_, count in ((0, H), (1, G)):
        if count > 0:
            all_sent(kbuf.at[0:count], kv_s.at[way_, 0])
            all_sent(vbuf.at[0:count], kv_s.at[way_, 1])
            all_sent(zagg.at[0:count], za_s.at[way_])
    if Y > 1:
        all_sent(yagg.at[0 : Y - 1], ya_s)
        all_sent(qbuf.at[0 : Y - 1], q_s)
        all_sent(stat.at[0 : Y - 1], st_s)
    all_sent(halo, halo_s)
    weights_step(jnp.int32(H + 2))
    total = own_c[...]
    all_here(pbuf.at[0 : Y - 1], cb_r)
    for d in range(1, Y):
        total = total + pbuf[(y + d) % Y].astype(F32)
    total = total * lax.rsqrt(jnp.mean(total * total, axis=0, keepdims=True) + EPS_HEAD)
    gate = gate_s[...].astype(F32)
    att = total.T * head_gain[...] * HEAD_FACTOR * (gate * jax.nn.sigmoid(gate))
    att_m[...] = att.astype(BF16)
    for d in range(1, 2 * X):
        share(att_m, att_g, am_s, am_r, d).start()

    weights_step(jnp.int32(H + 3))

    weights_here(0)
    left = shared(rec_m, rec_g, rm_s, rm_r)
    for q in parts_x:
        cols = slice(q * wide, (q + 1) * wide)
        out_a[:, cols] = jnp.dot(left, wfull[0, :, cols], preferred_element_type=F32)
    if H > 1:
        weights_here(1)
    left = shared(att_m, att_g, am_s, am_r)
    for q in parts_x:
        cols = slice(q * wide, (q + 1) * wide)
        part = jnp.dot(left, wfull[1, :, cols], preferred_element_type=F32)
        out[:, cols] = (out_a[:, cols] + part).astype(BF16)

    mine = pl.ds(pl.multiple_of(tp * WIDTH, WIDTH), WIDTH)
    for k in range(7):
        all_sent(wfull.at[:, mine, :], wg_s.at[k])
    for k in range(1, 7):
        all_sent(block(tp), ag_s.at[k])
    all_sent(pbuf.at[0 : Y - 1], cb_s)
    all_sent(rec_m.at[0 : (2 * X - 1) * rows, :], rm_s)
    all_sent(att_m.at[0 : (2 * X - 1) * rows, :], am_s)


def build(mesh, Y):
    SP, TP = mesh.shape["sp"], mesh.shape["tp"]
    Z, X = SP // Y, TP // 2

    def body(
        tokens, norm_gain, w_query, w_key, w_value, w_att_gate, w_rec_in, w_rec_gate, conv_taps,
        gate_recur, gate_input, decay_rate, head_lambda, head_gain, out_att, out_rec,
    ):
        rows, D = tokens.shape
        R = rows * TP
        H, G = Z // 2, max(Z - 1 - Z // 2, 1)
        vmem, far = pl.BlockSpec(memory_space=pltpu.VMEM), pl.BlockSpec(memory_space=pl.ANY)
        V, dma = pltpu.VMEM, pltpu.SemaphoreType.DMA
        scratch = [
            V((D, 6 * WIDTH), BF16), V((2, TP * WIDTH, D), BF16), V((R, D), BF16),
            V((Z, R, WIDTH), BF16), V((Z, WIDTH, R), BF16), V((Y, WIDTH, R), BF16),
            V((2 * Y, 2 * WIDTH, R), BF16), V((2 * Y, WIDTH, R), F32),
            V((2 * Y, R), F32), V((2 * Y, R), F32), V((2 * Y, R, R), BF16), V((2 * Y, R), F32),
            V((R, WIDTH), BF16), V((R, WIDTH), BF16), V((R, WIDTH), BF16),
            V((16, WIDTH), BF16), V((R + 16, WIDTH), F32),
            V((R, WIDTH), F32), V((R, WIDTH), F32), V((Y, 8, WIDTH), F32), V((Z, 8, WIDTH), F32),
            V((Y, 4 * Y, R), F32), V((Y, WIDTH, R), BF16), V((Y, WIDTH, R), BF16),
            V((WIDTH, R), F32), V((R, WIDTH), BF16), V((R, WIDTH), BF16),
            V((TP, rows, WIDTH), BF16), V((TP, rows, WIDTH), BF16), V((rows, D), F32),
            dma((8,)), dma((7,)), dma((X, PIECES)), dma((X,)), dma((2, 2)), dma((2 * HALVES, Z)),
            dma(()), dma(()), dma(()), dma(()), dma(()), dma(()), dma((2,)), dma((Z,)),
            dma(()), dma(()), dma(()), dma(()), dma((7,)), dma((X, H)), dma((2, X)),
            dma(()), dma(()), dma(()), dma(()),
        ]
        return pl.pallas_call(
            functools.partial(kernel, Z, Y, X),
            out_shape=jax.ShapeDtypeStruct((rows, D), BF16),
            in_specs=[vmem, vmem] + [far] * 6 + [vmem] * 6 + [far] * 2,
            out_specs=vmem,
            scratch_shapes=scratch,
            compiler_params=pltpu.CompilerParams(
                collective_id=0, has_side_effects=True, vmem_limit_bytes=56 * 1024 * 1024
            ),
        )(
            tokens, norm_gain.reshape(1, -1), w_query, w_key, w_value, w_att_gate, w_rec_in,
            w_rec_gate, conv_taps, gate_recur, gate_input, decay_rate.reshape(1, -1),
            head_lambda.reshape(1, 1), head_gain.reshape(1, -1), out_att, out_rec,
        )

    both = P(("sp", "tp"), None)
    cols, lead = P(None, "tp"), P("tp")
    placed = (
        both, P(), cols, cols, cols, cols, cols, cols, cols,
        P("tp", None, None), P("tp", None, None), lead, lead, lead, P("tp", None), P("tp", None),
    )
    return jax.shard_map(body, mesh=mesh, in_specs=placed, out_specs=both, check_vma=False)


def solution(mesh):
    return build(mesh, 4)
```
